32 devices in a mesh: kv: 16 (over z, y, core), tp: 2 (over x).
Axes of the slice: x: 2, y: 2, z: 4, core: 2. Of those that a mesh axis runs over, the one named last changes fastest.
Arguments:
- queries: bfloat16 [4096, 4, 128], P('kv', 'tp'), may hold values from -6 to 6
- keys: bfloat16 [4096, 4, 128], P('kv', 'tp'), may hold values from -6 to 6
- values: bfloat16 [4096, 4, 128], P('kv', 'tp'), may hold values from -6 to 6
- attended: bfloat16 [4096, 4, 128], P('kv', 'tp'), may hold values from -6 to 6
- out_grad: bfloat16 [4096, 4, 128], P('kv', 'tp'), may hold values from -6 to 6
- log_sum: float32 [4096, 4], P('kv', 'tp'), may hold values from 2.5 to 4.5
- picked: int32 [32, 16], P('kv'), may hold values from -1 to 127, as said below
- layer_input: bfloat16 [4096, 4096], P('kv'), may hold values from -0.03125 to 0.03125
Outputs:
- query_grad: float32 [4096, 4, 128], P('kv', 'tp')
- key_grad: float32 [4096, 4, 128], P('kv', 'tp')
- value_grad: float32 [4096, 4, 128], P('kv', 'tp')
- weight_grad: float32 [4096, 512], P('kv', 'tp')
The draws below stay inside these ranges and needn't reach their ends.
Inputs may be any that keep to these rules, and one draw needn't show every extreme that they name: Row r lists distinct key block numbers picked by query block r, followed by -1 to the end of the row; at least one entry is not -1, and at most 16 are. No picked block starts after the last position of its query block. With the span of a position being the position divided by 256 (rounded down), the span of every picked block is the query block's span or that span less 1, 2, 4, 8 and so on. The query blocks of one span pick at most 4 distinct blocks from any other single span.
All inputs are finite; a program needn't handle non-finite values.
Results may differ from the reference program's by a relative error of at most 0.004.
Values may be sent and summed in bfloat16 or wider, within the bound.
No kernel may reach another device: no remote copies, remote signals or barrier semaphores. Data moves between devices by JAX's collectives and lax.ppermute only.
A program may use at most 64 MiB of HBM per device.

```python
import jax
import jax.numpy as jnp
from jax import lax

D = 4096
HEADS = 4
DH = 128
TOK_DEV = 256
QB = 128
KB = 32
MAXSEL = 16
PER_SPAN = 4
TOKENS = 4096
QBLOCKS = 32


def draw_picked(key, part):
    span_count = TOKENS // TOK_DEV
    span_blocks = TOK_DEV // KB
    query_count = TOK_DEV // QB
    levels = span_count.bit_length() - 1
    groups = levels + 1
    slot_total = groups * span_blocks
    allow_key = jax.random.fold_in(key, 11)
    score_key = jax.random.fold_in(key, 12)
    count_key_a = jax.random.fold_in(key, 13)
    count_key_b = jax.random.fold_in(key, 14)
    block_axis = jnp.arange(span_blocks, dtype=jnp.int32)
    allow_scores = jax.random.randint(allow_key, (span_count, groups, span_blocks), 0, 1 << 20, dtype=jnp.int32) * span_blocks + block_axis
    allow_rank = jnp.argsort(jnp.argsort(allow_scores, axis=-1), axis=-1)
    allowed = allow_rank < PER_SPAN
    span_index = jnp.arange(span_count, dtype=jnp.int32)[:, None, None, None]
    query_index = jnp.arange(query_count, dtype=jnp.int32)[None, :, None, None]
    group_index = jnp.arange(groups, dtype=jnp.int32)[None, None, :, None]
    block_index = block_axis[None, None, None, :]
    back_spans = jnp.where(group_index == 0, 0, jnp.left_shift(jnp.ones_like(group_index), jnp.maximum(group_index - 1, 0)))
    owner_span = span_index - back_spans
    own_usable = (group_index == 0) & (block_index * KB <= query_index * QB + QB - 1)
    far_usable = (group_index > 0) & (owner_span >= 0) & allowed[:, None, :, :]
    usable = own_usable | far_usable
    slot_index = group_index * span_blocks + block_index
    draw_scores = jax.random.randint(score_key, (span_count, query_count, groups, span_blocks), 0, 1 << 16, dtype=jnp.int32)
    unique = draw_scores * slot_total + slot_index
    masked = jnp.where(usable, unique, -1)
    group_best = jnp.max(masked, axis=-1, keepdims=True)
    last_query = query_index == query_count - 1
    forced = usable & (masked == group_best) | usable & last_query & (group_index == 1)
    ranked = jnp.where(usable, unique + jnp.where(forced, 1 << 28, 0), -1)
    half_most = MAXSEL // 2
    extra_picks = jax.random.randint(count_key_a, (span_count, query_count), 0, half_most + 1, dtype=jnp.int32) * jax.random.randint(count_key_b, (span_count, query_count), 0, half_most + 1, dtype=jnp.int32) // half_most
    usable_count = jnp.sum(usable.astype(jnp.int32), axis=(2, 3))
    forced_count = jnp.sum(forced.astype(jnp.int32), axis=(2, 3))
    last_row = (jnp.arange(query_count, dtype=jnp.int32) == query_count - 1)[None, :]
    wanted = jnp.where(last_row, MAXSEL, jnp.maximum(half_most + extra_picks, forced_count))
    pick_count = jnp.minimum(wanted, usable_count)
    flat_ranked = ranked.reshape(span_count, query_count, slot_total)
    top_values, top_slots = lax.top_k(flat_ranked, MAXSEL)
    chosen_group = top_slots // span_blocks
    chosen_block = top_slots % span_blocks
    chosen_back = jnp.where(chosen_group == 0, 0, jnp.left_shift(jnp.ones_like(chosen_group), jnp.maximum(chosen_group - 1, 0)))
    chosen_span = jnp.arange(span_count, dtype=jnp.int32)[:, None, None] - chosen_back
    chosen_ids = chosen_span * span_blocks + chosen_block
    position = jnp.arange(MAXSEL, dtype=jnp.int32)[None, None, :]
    chosen_ids = jnp.where(position < pick_count[:, :, None], chosen_ids, -1)
    return chosen_ids.reshape(span_count * query_count, MAXSEL).astype(jnp.int32)


def raised(array, own_key, source, target, shards_of, factor):
    def block_of(axis_at):
        return (jnp.arange(array.shape[axis_at]) // (array.shape[axis_at] // shards_of)).reshape((-1,) + (1,) * (array.ndim - 1 - axis_at))

    one_side = jax.random.permutation(own_key, shards_of)[block_of(target)]
    other_side = (block_of(target) + shards_of // 2) % shards_of
    return jnp.where((block_of(source) == one_side) | (block_of(source) == other_side), factor * array, array)


def level_of(stream_key, extent, split, smallest, high):
    gain, own = 1.0, jax.random.fold_in(stream_key, 6)
    for axis_at, blocks in split:
        draws = jnp.exp(jax.random.uniform(jax.random.fold_in(own, axis_at), (blocks,), jnp.float32, smallest / len(split), high / len(split)))
        gain = gain * jnp.repeat(draws, extent[axis_at] // blocks).reshape([-1 if axis == axis_at else 1 for axis in range(len(extent))])
    return gain


def gaussian(rng, dims, scale, bound, split=(), kind=jnp.bfloat16):
    entries = scale * jax.random.normal(rng, dims, jnp.float32)
    if split:
        entries = entries * level_of(rng, dims, split, -0.22, 0.18)
    return jnp.clip(entries, -bound, bound).astype(kind)


def heavy_noise(key, extent, spread, bound, cuts, heavy, kind=jnp.bfloat16):
    entries = spread * jax.random.normal(key, extent, jnp.float32)
    if cuts:
        entries = entries * level_of(key, extent, cuts, -0.22, 0.18)
    return jnp.clip(raised(entries, jax.random.fold_in(key, 3), *heavy), -bound, bound).astype(kind)


def setup_inputs(seed: int = 0) -> dict:
    arg_keys = jax.random.split(jax.random.key(seed), 9)
    queries = gaussian(arg_keys[0], (TOKENS, HEADS, DH), 1.0, 6.0, ((0, 16), (1, 2)))
    keys = gaussian(arg_keys[1], (TOKENS, HEADS, DH), 1.0, 6.0, ((0, 16), (1, 2)))
    values = gaussian(arg_keys[2], (TOKENS, HEADS, DH), 1.0, 6.0, ((0, 16), (1, 2)))
    attended = gaussian(arg_keys[3], (TOKENS, HEADS, DH), 1.0, 6.0, ((0, 16), (1, 2)))
    out_grad = gaussian(arg_keys[4], (TOKENS, HEADS, DH), 1.0, 6.0, ((0, 16), (1, 2)))
    log_sum = jnp.clip(2.5 + 2.0 * jax.random.uniform(arg_keys[5], (TOKENS, HEADS), jnp.float32) ** level_of(arg_keys[5], (TOKENS, HEADS), ((0, 16), (1, 2)), -0.2, 0.2), 2.5, 4.5)
    picked = draw_picked(jax.random.fold_in(arg_keys[8], 71), 0)
    layer_input = heavy_noise(arg_keys[7], (TOKENS, D), 0.004, 0.03125, ((0, 16),), (0, 1, 16, 2.0))
    return dict(queries=queries, keys=keys, values=values, attended=attended, out_grad=out_grad, log_sum=log_sum, picked=picked, layer_input=layer_input)


def reference(queries, keys, values, attended, out_grad, log_sum, picked, layer_input):
    score_scale = DH ** -0.5
    row_dots = jnp.sum(out_grad.astype(jnp.float32) * attended.astype(jnp.float32), axis=-1)
    key_offsets = jnp.arange(KB, dtype=jnp.int32)
    query_offsets = jnp.arange(QB, dtype=jnp.int32)

    def one_block(carry, block_index):
        key_sums, value_sums = carry
        listed = picked[block_index]
        listed_live = listed >= 0
        gather_rows = (jnp.where(listed_live, listed, 0)[:, None] * KB + key_offsets[None, :]).reshape(-1).astype(jnp.int32)
        key_live = jnp.repeat(listed_live, KB)
        first_query = (block_index * QB).astype(jnp.int32)
        query_pos = first_query + query_offsets
        pair_live = key_live[None, :] & (gather_rows[None, :] <= query_pos[:, None])
        query_rows = lax.dynamic_slice_in_dim(queries, first_query, QB, 0).astype(jnp.float32)
        grad_rows = lax.dynamic_slice_in_dim(out_grad, first_query, QB, 0).astype(jnp.float32)
        stored = lax.dynamic_slice_in_dim(log_sum, first_query, QB, 0)
        block_dots = lax.dynamic_slice_in_dim(row_dots, first_query, QB, 0)
        key_rows = keys[gather_rows].astype(jnp.float32)
        value_rows = values[gather_rows].astype(jnp.float32)
        scores = jnp.einsum("qhd,khd->hqk", query_rows, key_rows) * score_scale
        weights = jnp.where(pair_live[None], jnp.exp(scores - stored.T[:, :, None]), 0.0)
        slopes = jnp.einsum("qhd,khd->hqk", grad_rows, value_rows)
        score_grad = weights * (slopes - block_dots.T[:, :, None])
        weight_pairs = lax.optimization_barrier(weights.astype(jnp.bfloat16)).astype(jnp.float32)
        grad_pairs = lax.optimization_barrier(score_grad.astype(jnp.bfloat16)).astype(jnp.float32)
        query_grad = jnp.einsum("hqk,khd->qhd", grad_pairs, key_rows) * score_scale
        key_terms = jnp.einsum("hqk,qhd->khd", grad_pairs, query_rows) * score_scale
        value_terms = jnp.einsum("hqk,qhd->khd", weight_pairs, grad_rows)
        key_sums = key_sums.at[gather_rows].add(key_terms)
        value_sums = value_sums.at[gather_rows].add(value_terms)
        return (key_sums, value_sums), query_grad

    empty = jnp.zeros(keys.shape, jnp.float32)
    (key_grad, value_grad), query_grad = lax.scan(one_block, (empty, empty), jnp.arange(QBLOCKS, dtype=jnp.int32))
    query_grad = query_grad.reshape(TOKENS, HEADS, DH)
    value_round = value_grad.astype(jnp.bfloat16).reshape(TOKENS, HEADS * DH)
    weight_grad = lax.dot_general(layer_input, value_round, (((0,), (0,)), ((), ())), preferred_element_type=jnp.float32)
    return query_grad, key_grad, value_grad, weight_grad
```

```python
import functools

import jax
import jax.numpy as jnp
from jax import lax
from jax.experimental import pallas as pl
from jax.experimental.pallas import tpu as pltpu
from jax.sharding import PartitionSpec as P

QB = 128
KB = 32
F32 = jnp.float32
BF16 = jnp.bfloat16
VMEM = pl.BlockSpec(memory_space=pltpu.VMEM)
SMEM = pl.BlockSpec(memory_space=pltpu.SMEM)


def ring(value, by):
    count = lax.axis_size("kv")
    return lax.ppermute(value, "kv", [(i, (i + by) % count) for i in range(count)])


def swap(value, bit):
    count = lax.axis_size("kv")
    return lax.ppermute(value, "kv", [(i, i ^ bit) for i in range(count)])


def call(body, out_shape, specs, flops, nbytes):
    return pl.pallas_call(
        body,
        out_shape=out_shape,
        in_specs=specs,
        out_specs=jax.tree.map(lambda _: VMEM, out_shape),
        cost_estimate=pl.CostEstimate(flops=flops, bytes_accessed=nbytes, transcendentals=0),
    )


def nt(a, b):
    return lax.dot_general(a, b, (((1,), (1,)), ((), ())), preferred_element_type=F32)


def tn(a, b):
    return lax.dot_general(a, b, (((0,), (0,)), ((), ())), preferred_element_type=F32)


def nn(a, b):
    return lax.dot_general(a, b, (((1,), (0,)), ((), ())), preferred_element_type=F32)


def layout(tok, heads, sel):
    blocks = tok // QB
    codes = 2 * heads * tok
    stats = codes + blocks * sel
    per = -(-6 * heads // 16) * 16
    return blocks, codes, stats, per, stats + blocks * per


def thirds(row):
    high = row.astype(BF16).astype(F32)
    rest = row - high
    middle = rest.astype(BF16).astype(F32)
    return [high, middle, rest - middle]


def pack_body(levels, me_ref, picked_ref, q_ref, g_ref, a_ref, lse_ref, msg_ref):
    tok, heads, dim = q_ref.shape
    sel = picked_ref.shape[1]
    span_blocks = tok // KB
    blocks, codes, stats, per, _ = layout(tok, heads, sel)
    me = me_ref[0]
    rows = lax.broadcasted_iota(jnp.int32, (sel, QB), 0)
    for b in range(blocks):
        code = jnp.full((sel, QB), -1, jnp.int32)
        for p in range(sel):
            block = picked_ref[b, p]
            span = lax.div(jnp.maximum(block, 0), span_blocks)
            group = jnp.int32(0)
            for level in range(levels):
                group += ((me - span) >= (1 << level)).astype(jnp.int32)
            value = jnp.where(block < 0, -1, group * span_blocks + block - span * span_blocks)
            code = jnp.where(rows == p, value, code)
        msg_ref[codes + b * sel : codes + (b + 1) * sel, :] = code.astype(F32).astype(BF16)
    table = [[] for _ in range(blocks)]
    for h in range(heads):
        query = q_ref[:, h, :]
        grad = g_ref[:, h, :]
        msg_ref[h * tok : (h + 1) * tok, :] = query
        msg_ref[(heads + h) * tok : (heads + h + 1) * tok, :] = grad
        product = grad.astype(F32) * a_ref[:, h, :].astype(F32)
        for b in range(blocks):
            part = product[b * QB : (b + 1) * QB, :]
            dots = jnp.sum(part.T, axis=0, keepdims=True)
            table[b] += thirds(lse_ref[h : h + 1, b * QB : (b + 1) * QB]) + thirds(dots)
    for b in range(blocks):
        at = stats + b * per
        filled = table[b] + [jnp.zeros((per - 6 * heads, QB), F32)]
        msg_ref[at : at + per, :] = jnp.concatenate(filled, axis=0).astype(BF16)


def unsplit(rows):
    return (rows[0:1] + rows[1:2]) + rows[2:3]


def group_terms(msg_ref, key_of, value_of, group, tok, heads, dim, sel, causal, out):
    blocks, codes, stats, per, _ = layout(tok, heads, sel)
    span_blocks = tok // KB
    scale = dim ** (-0.5)
    lives, lse, dots = [], [[] for _ in range(heads)], [[] for _ in range(heads)]
    for b in range(blocks):
        code = msg_ref[codes + b * sel : codes + (b + 1) * sel, :].astype(F32)
        rows = []
        for k in range(span_blocks):
            hit = jnp.max(jnp.where(code == float(group * span_blocks + k), 1.0, 0.0), axis=0, keepdims=True)
            rows.append(jnp.broadcast_to(hit, (KB, QB)))
        lives.append(jnp.concatenate(rows, axis=0))
        stat = msg_ref[stats + b * per : stats + (b + 1) * per, :].astype(F32)
        for h in range(heads):
            lse[h].append(unsplit(stat[6 * h : 6 * h + 3]))
            dots[h].append(unsplit(stat[6 * h + 3 : 6 * h + 6]))
    live = jnp.concatenate(lives, axis=1) > 0.5
    if causal:
        key_pos = lax.broadcasted_iota(jnp.int32, (tok, tok), 0)
        query_pos = lax.broadcasted_iota(jnp.int32, (tok, tok), 1)
        live = live & (key_pos <= query_pos)
    for h in range(heads):
        query = msg_ref[h * tok : (h + 1) * tok, :]
        grad = msg_ref[(heads + h) * tok : (heads + h + 1) * tok, :]
        key, value = key_of(h), value_of(h)
        scores = nt(key, query) * scale
        weights = jnp.where(live, jnp.exp(scores - jnp.concatenate(lse[h], axis=1)), 0.0)
        slopes = nt(value, grad)
        score_grad = weights * (slopes - jnp.concatenate(dots[h], axis=1))
        weight_pairs = weights.astype(BF16)
        grad_pairs = score_grad.astype(BF16)
        out(h, nn(grad_pairs, query), nn(weight_pairs, grad), tn(grad_pairs, key))


def own_body(sel, msg_ref, k_ref, v_ref, kv_ref, dk_ref, dv_ref, dq_ref):
    tok, heads, dim = k_ref.shape
    for h in range(heads):
        kv_ref[h * tok : (h + 1) * tok, :] = k_ref[:, h, :]
        kv_ref[(heads + h) * tok : (heads + h + 1) * tok, :] = v_ref[:, h, :]

    def out(h, dk, dv, dq):
        at = slice(h * tok, (h + 1) * tok)
        dk_ref[at, :] = dk
        dv_ref[at, :] = dv
        dq_ref[at, :] = dq

    group_terms(
        msg_ref,
        lambda h: kv_ref[h * tok : (h + 1) * tok, :],
        lambda h: kv_ref[(heads + h) * tok : (heads + h + 1) * tok, :],
        0, tok, heads, dim, sel, True, out,
    )


def far_body(sel, tok, heads, groups, *refs):
    count = len(groups)
    msgs = refs[:count]
    kv_ref, dk_in, dv_in = refs[count : count + 3]
    dk_out, dv_out, round_ref = refs[count + 3 : count + 6]
    dqs = refs[count + 6 : count + 6 + count]
    dk_sum, dv_sum = refs[count + 6 + count :]
    dim = kv_ref.shape[1]
    scale = dim ** (-0.5)
    for index, group in enumerate(groups):

        def out(h, dk, dv, dq):
            at = slice(h * tok, (h + 1) * tok)
            dk_sum[at, :] = (dk_sum if index else dk_in)[at, :] + dk
            dv_sum[at, :] = (dv_sum if index else dv_in)[at, :] + dv
            dqs[index][at, :] = dq.astype(BF16)

        group_terms(
            msgs[index],
            lambda h: kv_ref[h * tok : (h + 1) * tok, :],
            lambda h: kv_ref[(heads + h) * tok : (heads + h + 1) * tok, :],
            group, tok, heads, dim, sel, False, out,
        )
    for h in range(heads):
        at = slice(h * tok, (h + 1) * tok)
        dk_out[:, h, :] = dk_sum[at, :] * scale
        dv = dv_sum[at, :]
        dv_out[:, h, :] = dv
        round_ref[:, h * dim : (h + 1) * dim] = dv.astype(BF16)


def query_body(dq_ref, *refs):
    out_ref = refs[-1]
    tok, heads, dim = out_ref.shape
    scale = dim ** (-0.5)
    for h in range(heads):
        at = slice(h * tok, (h + 1) * tok)
        total = dq_ref[at, :]
        for ref in refs[:-1]:
            total = total + ref[at, :].astype(F32)
        out_ref[:, h, :] = total * scale


def pieces_body(near, far, me_ref, x_ref, *out_refs):
    rank = lax.rem(me_ref[0], near)
    width = x_ref.shape[1] // (near * far)
    for index, ref in enumerate(out_refs):
        target = rank ^ (index + 1)
        for z in range(far):
            at = pl.multiple_of((z * near + target) * width, width)
            ref[:, z * width : (z + 1) * width] = x_ref[:, pl.ds(at, width)]


def weight_body(near, far, parity, out_type, me_ref, x_ref, *refs):
    pieces = refs[: near - 1]
    rounds_ref, out_ref = refs[near - 1 :]
    me = me_ref[0]
    rank, depth = lax.rem(me, near), lax.div(me, near)
    tok = x_ref.shape[0]
    width = x_ref.shape[1] // (near * far)
    step = 2 if parity is not None else 1
    for index, rel in enumerate(range(parity or 0, far, step)):
        z = depth ^ rel
        at = pl.multiple_of((z * near + rank) * width, width)
        total = tn(x_ref[:, pl.ds(at, width)], rounds_ref[pl.ds(pl.multiple_of(rank * tok, tok), tok), :])
        for m in range(1, near):
            left = pieces[m - 1][:, pl.ds(pl.multiple_of(z * width, width), width)]
            right = rounds_ref[pl.ds(pl.multiple_of((rank ^ m) * tok, tok), tok), :]
            total += tn(left, right)
        out_ref[index * width : (index + 1) * width, :] = total.astype(out_type)


def per_device(queries, keys, values, attended, out_grad, log_sum, picked, layer_input):
    tok, heads, dim = queries.shape
    sel = picked.shape[1]
    count = lax.axis_size("kv")
    levels = count.bit_length() - 1
    near = 1 << (levels // 2)
    far = count // near
    me = lax.axis_index("kv").astype(jnp.int32).reshape(1)
    rows = heads * tok
    msg_rows = layout(tok, heads, sel)[-1]

    def shape(dims, kind):
        return jax.ShapeDtypeStruct(dims, kind)

    pairs = tok * tok * dim * heads * 10
    msg = call(
        functools.partial(pack_body, levels),
        shape((msg_rows, dim), BF16),
        [SMEM, SMEM, VMEM, VMEM, VMEM, VMEM],
        1 << 20, 4 * rows * dim * 2,
    )(me, picked, queries, out_grad, attended, log_sum.T)
    got = [ring(msg, -(1 << level)) for level in range(levels)]
    width = layer_input.shape[1] // count
    blocked = width % 128 == 0 and far > 1
    if blocked:
        sent = call(
            functools.partial(pieces_body, near, far),
            [shape((tok, far * width), BF16)] * (near - 1),
            [SMEM, VMEM],
            1 << 20, 2 * layer_input.size * 2,
        )(me, layer_input)
        pieces = [swap(piece, m + 1) for m, piece in enumerate(sent)]
    kv, dk_own, dv_own, dq_own = call(
        functools.partial(own_body, sel),
        [shape((2 * rows, dim), BF16)] + [shape((rows, dim), F32)] * 3,
        [VMEM] * 3,
        pairs, 8 * rows * dim * 4,
    )(msg, keys, values)
    groups = tuple(range(1, levels + 1))
    outs = pl.pallas_call(
        functools.partial(far_body, sel, tok, heads, groups),
        out_shape=[shape((tok, heads, dim), F32)] * 2
        + [shape((tok, heads * dim), BF16)]
        + [shape((rows, dim), BF16)] * levels,
        in_specs=[VMEM] * (levels + 3),
        out_specs=[VMEM] * (levels + 3),
        scratch_shapes=[pltpu.VMEM((rows, dim), F32)] * 2,
        cost_estimate=pl.CostEstimate(
            flops=pairs * levels, bytes_accessed=levels * 8 * rows * dim, transcendentals=0
        ),
    )(*got, kv, dk_own, dv_own)
    key_grad, value_grad, rounded = outs[:3]
    sides = outs[3:]
    if blocked:
        bunches = [[g * near + r for r in range(near)] for g in range(far)]
        rounds = lax.all_gather(rounded, "kv", axis_index_groups=bunches, tiled=True)

        def weight(parity, kind):
            blocks = far // 2 if parity is not None else far
            return call(
                functools.partial(weight_body, near, far, parity, kind),
                shape((blocks * width, heads * dim), kind),
                [SMEM] + [VMEM] * (near + 1),
                2 * near * tok * blocks * width * heads * dim, layer_input.size * 2,
            )(me, layer_input, *pieces, rounds)

        send = weight(1, BF16)
        keep = weight(0, F32)
        bit = near
        total = keep + swap(send, bit).astype(F32)
        left = far // 2
        while left > 1:
            bit *= 2
            stacked = total.reshape(left // 2, 2, width, heads * dim)
            send = stacked[:, 1].reshape(-1, heads * dim).astype(BF16)
            total = stacked[:, 0].reshape(-1, heads * dim) + swap(send, bit).astype(F32)
            left //= 2
    else:
        terms = lax.dot_general(
            layer_input, rounded, (((0,), (0,)), ((), ())), preferred_element_type=F32
        )
        total = lax.psum_scatter(terms, "kv", scatter_dimension=0, tiled=True)
    back = [ring(side, 1 << level) for level, side in enumerate(sides)]
    query_grad = call(
        query_body, shape((tok, heads, dim), F32), [VMEM] * (levels + 1), 1 << 20, rows * dim * 16
    )(dq_own, *back)
    return query_grad, key_grad, value_grad, total


def solution(mesh):
    placed = (
        P("kv", "tp", None),
        P("kv", "tp", None),
        P("kv", "tp", None),
        P("kv", "tp", None),
        P("kv", "tp", None),
        P("kv", "tp"),
        P("kv", None),
        P("kv", None),
    )
    return jax.shard_map(
        per_device,
        mesh=mesh,
        in_specs=placed,
        out_specs=(P("kv", "tp", None), P("kv", "tp", None), P("kv", "tp", None), P("kv", "tp")),
        check_vma=False,
    )
```

```python
import functools

import jax
import jax.numpy as jnp
from jax import lax
from jax.experimental import pallas as pl
from jax.experimental.pallas import tpu as pltpu
from jax.sharding import PartitionSpec as P


QB = 128
KB = 32
LIMIT = 12 << 20
F32 = jnp.float32
BF16 = jnp.bfloat16
VMEM = pl.BlockSpec(memory_space=pltpu.VMEM)
HBM = pl.BlockSpec(memory_space=pltpu.HBM)


def ring(value, by):
    count = lax.axis_size("kv")
    return lax.ppermute(value, "kv", [(i, (i + by) % count) for i in range(count)])


def swap(value, bit):
    count = lax.axis_size("kv")
    return lax.ppermute(value, "kv", [(i, i ^ bit) for i in range(count)])


def forward(msg, levels, mix):
    if levels < 4:
        return [ring(msg, -(1 << level)) for level in range(levels)]
    four = ring(msg, -4)
    eight = ring(four, -4)
    payload = mix(2, msg, four)
    two = swap(payload, 2)
    payload = mix(1, msg, two)
    one = swap(payload, 1)
    return [one, two, four, eight] + [ring(msg, -(1 << level)) for level in range(4, levels)]


def call(body, out_shape, specs, flops, nbytes, local=True):
    kept = jax.tree.map(lambda x: pltpu.VMEM(x.shape, x.dtype) if local else x, out_shape)
    return pl.pallas_call(
        body,
        out_shape=kept,
        in_specs=specs,
        out_specs=jax.tree.map(lambda _: VMEM, out_shape),
        cost_estimate=pl.CostEstimate(flops=flops, bytes_accessed=nbytes, transcendentals=0),
        compiler_params=pltpu.CompilerParams(vmem_limit_bytes=LIMIT),
    )


def nt(a, b):
    return lax.dot_general(a, b, (((1,), (1,)), ((), ())), preferred_element_type=F32)


def tn(a, b):
    return lax.dot_general(a, b, (((0,), (0,)), ((), ())), preferred_element_type=F32)


def nn(a, b):
    return lax.dot_general(a, b, (((1,), (0,)), ((), ())), preferred_element_type=F32)


PER = 8
BIG = 16384.0
LOG2E = 1.4426950408889634


def layout(tok, heads, sel):
    rows = heads * tok
    codes = 2 * rows
    stats = codes + tok // QB * sel
    return rows, codes, stats, stats + rows // 128 * PER


def thirds(row):
    high = row.astype(BF16)
    rest = row - high.astype(F32)
    middle = rest.astype(BF16)
    return high, middle, (rest - middle.astype(F32)).astype(BF16)


def pack_body(levels, heads, picked_hbm, q_hbm, g_hbm, a_hbm, lse_hbm, msg_ref, picked_ref, a_ref, lse_ref, sem):
    rows = q_hbm.shape[0]
    tok = rows // heads
    sel = picked_ref.shape[1]
    span_blocks = tok // KB
    blocks = tok // QB
    _, codes, stats, _ = layout(tok, heads, sel)
    copies = [
        pltpu.make_async_copy(picked_hbm, picked_ref, sem.at[0]),
        pltpu.make_async_copy(lse_hbm, lse_ref, sem.at[1]),
        pltpu.make_async_copy(g_hbm, msg_ref.at[rows : 2 * rows, :], sem.at[2]),
        pltpu.make_async_copy(a_hbm, a_ref, sem.at[3]),
        pltpu.make_async_copy(q_hbm, msg_ref.at[0:rows, :], sem.at[4]),
    ]
    for copy in copies:
        copy.start()
    me = lax.axis_index("kv")
    copies[0].wait()
    order = lax.broadcasted_iota(jnp.int32, (sel, QB), 0)
    for b in range(blocks):
        code = jnp.full((sel, QB), -1, jnp.int32)
        for p in range(sel):
            block = picked_ref[b, p]
            span = lax.div(jnp.maximum(block, 0), span_blocks)
            group = jnp.int32(0)
            for level in range(levels):
                group += ((me - span) >= (1 << level)).astype(jnp.int32)
            value = jnp.where(block < 0, -1, group * span_blocks + block - span * span_blocks)
            code = jnp.where(order == p, value, code)
        msg_ref[codes + b * sel : codes + (b + 1) * sel, :] = code.astype(F32).astype(BF16)
    copies[1].wait()
    source = lax.broadcasted_iota(jnp.int32, (tok, rows), 0)
    target = lax.broadcasted_iota(jnp.int32, (tok, rows), 1)
    logs = jnp.zeros((PER, rows), F32)
    empty = jnp.zeros((PER - 3, tok), BF16)
    for h in range(heads):
        spread = jnp.where(target == source * heads + h, 1.0, 0.0).astype(BF16)
        parts = jnp.concatenate(list(thirds(lse_ref[h : h + 1, :])) + [empty], axis=0)
        logs += nn(parts, spread)
    copies[2].wait()
    copies[3].wait()
    product = msg_ref[rows : 2 * rows, :].astype(F32) * a_ref[...].astype(F32)
    ones = jnp.ones((PER, product.shape[1]), BF16)
    dots = sum(nt(ones, part) for part in thirds(product))
    split = [part.astype(F32) for part in thirds(dots)]
    row = lax.broadcasted_iota(jnp.int32, (PER, rows), 0)
    table = jnp.where(row < 3, logs, jnp.where(row == 3, split[0], jnp.where(row == 4, split[1], split[2])))
    table = jnp.where(row < 6, table, 0.0).astype(BF16)
    for c in range(rows // 128):
        msg_ref[stats + c * PER : stats + (c + 1) * PER, :] = table[:, c * 128 : (c + 1) * 128]
    copies[4].wait()


def unsplit(rows):
    return (rows[0:1] + rows[1:2]) + rows[2:3]


def group_terms(msg_ref, key, value, group, heads, sel, causal):
    rows, dim = key.shape
    tok = rows // heads
    _, codes, stats, _ = layout(tok, heads, sel)
    span_blocks = tok // KB
    chunks = QB * heads // 128
    dead = [[] for _ in range(span_blocks)]
    lse, dots = [], []
    for b in range(tok // QB):
        code = msg_ref[codes + b * sel : codes + (b + 1) * sel, :].astype(F32)
        for k in range(span_blocks):
            hit = jnp.where(code == float(group * span_blocks + k), 0.0, BIG)
            dead[k] += [jnp.min(hit, axis=0, keepdims=True)] * chunks
    for c in range(rows // 128):
        stat = msg_ref[stats + c * PER : stats + (c + 1) * PER, :].astype(F32)
        lse.append(unsplit(stat[0:3]))
        dots.append(unsplit(stat[3:6]))
    lse = jnp.concatenate(lse, axis=1) * LOG2E
    dots = jnp.concatenate(dots, axis=1)
    down = lax.broadcasted_iota(jnp.int32, (8, rows), 0)
    along = lax.broadcasted_iota(jnp.int32, (8, rows), 1)
    base = jnp.where(lax.rem(down, heads) == lax.rem(along, heads), 0.0, BIG) + lse
    shift = jnp.stack([base + jnp.concatenate(dead[k], axis=1) for k in range(span_blocks)])
    query = msg_ref[0:rows, :]
    grad = msg_ref[rows : 2 * rows, :]
    scores = nt(key, query) * (dim ** (-0.5) * LOG2E)
    scores = scores.reshape(span_blocks, KB * heads // 8, 8, rows) - shift[:, None]
    scores = scores.reshape(rows, rows)
    if causal:
        key_pos = lax.broadcasted_iota(jnp.int32, (rows, rows), 0)
        query_pos = lax.broadcasted_iota(jnp.int32, (rows, rows), 1)
        scores = jnp.where(lax.div(key_pos, heads) <= lax.div(query_pos, heads), scores, -BIG)
    weights = jnp.exp2(scores)
    score_grad = weights * (nt(value, grad) - dots)
    weight_pairs = weights.astype(BF16)
    grad_pairs = score_grad.astype(BF16)
    return nn(grad_pairs, query), nn(weight_pairs, grad), tn(grad_pairs, key)


def own_body(sel, heads, msg_ref, k_ref, v_ref, dk_ref, dv_ref, dq_ref):
    dk_ref[...], dv_ref[...], dq_ref[...] = group_terms(msg_ref, k_ref[...], v_ref[...], 0, heads, sel, True)


def far_body(sel, heads, groups, last, *refs):
    count = len(groups)
    msgs = refs[:count]
    k_ref, v_ref, dk_in, dv_in = refs[count : count + 4]
    dqs = refs[count + 4 : 2 * count + 4]
    dk_out, dv_out = refs[2 * count + 4 : 2 * count + 6]
    rows, dim = k_ref.shape
    scale = dim ** (-0.5)
    dk, dv = dk_in[...], dv_in[...]
    for index, group in enumerate(groups):
        dk_term, dv_term, dq = group_terms(msgs[index], k_ref[...], v_ref[...], group, heads, sel, False)
        dk, dv = dk + dk_term, dv + dv_term
        dqs[index][...] = dq.astype(BF16)
    dv_out[...] = dv
    if not last:
        dk_out[...] = dk
        return
    round_ref = refs[-1]
    for h in range(heads):
        at = pl.ds(h, rows // heads, stride=heads) if heads > 1 else slice(None)
        round_ref[:, h * dim : (h + 1) * dim] = dv_out[at, :].astype(BF16)
    dk_out[...] = dk * scale


def query_body(dq_ref, *refs):
    out_ref = refs[-1]
    total = dq_ref[...]
    for ref in refs[:-1]:
        total = total + ref[...].astype(F32)
    out_ref[...] = total * (out_ref.shape[1] ** (-0.5))


def mix_body(bit, yes_ref, no_ref, out_ref):
    picked = (lax.axis_index("kv") & bit) != 0

    @pl.when(picked)
    def _():
        out_ref[...] = yes_ref[...]

    @pl.when(jnp.logical_not(picked))
    def _():
        out_ref[...] = no_ref[...]


def share_of(tok, m, tp):
    return tok // tp if m > 1 and tok % (16 * tp) == 0 else tok


def cut_body(near, far, x_hbm, *refs):
    out_refs, sem = refs[:-1], refs[-1]
    rank = lax.rem(lax.axis_index("kv"), near)
    width = x_hbm.shape[1] // (near * far)
    copies = []
    for m in [*range(1, near), 0]:
        share = out_refs[m].shape[0]
        rows = slice(None)
        if share < x_hbm.shape[0]:
            rows = pl.ds(pl.multiple_of(lax.axis_index("tp") * share, share), share)
        for z in range(far):
            at = pl.multiple_of((z * near + (rank ^ m)) * width, width)
            copies.append(
                pltpu.make_async_copy(
                    x_hbm.at[rows, pl.ds(at, width)],
                    out_refs[m].at[:, z * width : (z + 1) * width],
                    sem.at[m * far + z],
                )
            )
    for copy in copies:
        copy.start()
    for copy in copies:
        copy.wait()


def weight_body(near, far, parity, counts, *refs):
    pieces = refs[: sum(counts)]
    rounds_ref, out_ref = refs[sum(counts) :]
    me = lax.axis_index("kv")
    rank, depth = lax.rem(me, near), lax.div(me, near)
    tok = rounds_ref.shape[0] // near
    width = pieces[0].shape[1] // far
    step = 2 if parity is not None else 1
    rights = []
    for m in range(near):
        for s in range(counts[m]):
            share = tok // counts[m]
            at = (rank ^ m) * tok + lax.rem(lax.axis_index("tp") + s, counts[m]) * share
            rights.append(rounds_ref[pl.ds(pl.multiple_of(at, share), share), :])
    right = jnp.concatenate(rights, axis=0)
    for index, rel in enumerate(range(parity or 0, far, step)):
        at = pl.multiple_of((depth ^ rel) * width, width)
        left = jnp.concatenate([piece[:, pl.ds(at, width)] for piece in pieces], axis=0)
        out_ref[index * width : (index + 1) * width, :] = tn(left, right).astype(out_ref.dtype)


def halve_body(blocks, keep_ref, came_ref, rest_ref, send_ref):
    width = keep_ref.shape[0] // blocks
    for block in range(blocks):
        at = slice(block * width, (block + 1) * width)
        to = slice(block // 2 * width, (block // 2 + 1) * width)
        total = keep_ref[at, :] + came_ref[at, :].astype(F32)
        if block % 2:
            send_ref[to, :] = total.astype(BF16)
        else:
            rest_ref[to, :] = total


def add_body(keep_ref, came_ref, out_ref):
    out_ref[...] = keep_ref[...] + came_ref[...].astype(F32)


def per_device(queries, keys, values, attended, out_grad, log_sum, picked, layer_input):
    tok, heads, dim = queries.shape
    sel = picked.shape[1]
    count = lax.axis_size("kv")
    levels = count.bit_length() - 1
    near = 1 << (levels // 2)
    far = count // near
    tp = lax.axis_size("tp")
    rows, _, _, msg_rows = layout(tok, heads, sel)
    flat = lambda x: x.reshape(rows, dim)
    key, value = flat(keys), flat(values)

    def shape(dims, kind):
        return jax.ShapeDtypeStruct(dims, kind)

    pairs = rows * rows * dim * 10
    msg = pl.pallas_call(
        functools.partial(pack_body, levels, heads),
        out_shape=pltpu.VMEM((msg_rows, dim), BF16),
        in_specs=[HBM] * 5,
        out_specs=VMEM,
        scratch_shapes=[
            pltpu.SMEM(picked.shape, jnp.int32),
            pltpu.VMEM((rows, dim), BF16),
            pltpu.VMEM((heads, tok), F32),
            pltpu.SemaphoreType.DMA((5,)),
        ],
        compiler_params=pltpu.CompilerParams(vmem_limit_bytes=62000000),
    )(picked, flat(queries), flat(out_grad), flat(attended), log_sum.T)

    def mix(bit, yes, no):
        return call(
            functools.partial(mix_body, bit), shape(yes.shape, BF16), [VMEM, VMEM], 1 << 18, yes.size * 6
        )(yes, no)

    got = forward(msg, levels, mix)
    width = layer_input.shape[1] // count
    blocked = width % 128 == 0 and far > 1
    if blocked:
        shares = [share_of(tok, m, tp) for m in range(near)]
        cuts = pl.pallas_call(
            functools.partial(cut_body, near, far),
            out_shape=[pltpu.VMEM((share, far * width), BF16) for share in shares],
            in_specs=[HBM],
            out_specs=[VMEM] * near,
            scratch_shapes=[pltpu.SemaphoreType.DMA((near * far,))],
            cost_estimate=pl.CostEstimate(flops=1 << 20, bytes_accessed=layer_input.size, transcendentals=0),
            compiler_params=pltpu.CompilerParams(vmem_limit_bytes=56 << 20),
        )(layer_input)
        pieces, counts = [cuts[0]], [1]
        for m in range(1, near):
            pieces.append(swap(cuts[m], m))
            counts.append(tok // shares[m])
            first = pieces[-1]
            for s in range(1, counts[m]):
                pieces.append(lax.ppermute(first, "tp", [((i + s) % tp, i) for i in range(tp)]))
    dk_own, dv_own, dq_own = call(
        functools.partial(own_body, sel, heads),
        [shape((rows, dim), F32)] * 3,
        [VMEM] * 3,
        pairs, 8 * rows * dim * 4,
    )(msg, key, value)

    def far_call(groups, dk, dv, last):
        kinds = [shape((rows, dim), BF16)] * len(groups) + [shape((rows, dim), F32)] * 2
        if last:
            kinds.append(shape((tok, heads * dim), BF16))
        return call(
            functools.partial(far_body, sel, heads, groups, last),
            kinds,
            [VMEM] * (len(groups) + 4),
            pairs * len(groups), 8 * rows * dim, not last,
        )(*[got[group - 1] for group in groups], key, value, dk, dv)

    back, dk, dv = {}, dk_own, dv_own
    stages = [(3,), (2,), (4,), (1,)] + [(level,) for level in range(5, levels + 1)]
    if levels < 4:
        stages = [tuple(range(1, levels + 1))]
    elif levels > 4:
        stages = [(level,) for level in range(1, levels + 1)]
    for stage in stages:
        outs = far_call(stage, dk, dv, stage == stages[-1])
        for group, side in zip(stage, outs):
            back[group] = ring(side, 1 << (group - 1))
        outs = outs[len(stage) :]
        dk, dv = outs[:2]
    key_grad, value_grad, rounded = outs
    if blocked:
        bunches = [[g * near + r for r in range(near)] for g in range(far)]
        rounds = lax.all_gather(rounded, "kv", axis_index_groups=bunches, tiled=True)

        columns = heads * dim

        def weight(parity, kind):
            blocks = far // 2
            return call(
                functools.partial(weight_body, near, far, parity, counts),
                shape((blocks * width, columns), kind),
                [VMEM] * (len(pieces) + 1),
                2 * near * tok * blocks * width * columns, near * tok * far * width * 2,
            )(*pieces, rounds)

        send = weight(1, BF16)
        total = weight(0, F32)
        bit, left = near, far // 2
        came = swap(send, bit)
        while left > 1:
            bit *= 2
            total, send = call(
                functools.partial(halve_body, left),
                [shape((left // 2 * width, columns), F32), shape((left // 2 * width, columns), BF16)],
                [VMEM] * 2, 1 << 18, left * width * columns * 8,
            )(total, came)
            left //= 2
            came = swap(send, bit)
        total = call(add_body, shape(total.shape, F32), [VMEM] * 2, 1 << 18, total.size * 10, False)(total, came)
    else:
        terms = lax.dot_general(
            layer_input, rounded, (((0,), (0,)), ((), ())), preferred_element_type=F32
        )
        total = lax.psum_scatter(terms, "kv", scatter_dimension=0, tiled=True)
    query_grad = call(
        query_body, shape((rows, dim), F32), [VMEM] * (levels + 1), 1 << 20, rows * dim * 16, False
    )(dq_own, *[back[group] for group in range(1, levels + 1)])
    grads = [x.reshape(tok, heads, dim) for x in (query_grad, key_grad, value_grad)]
    return (*grads, total)


def solution(mesh):
    placed = (
        P("kv", "tp", None),
        P("kv", "tp", None),
        P("kv", "tp", None),
        P("kv", "tp", None),
        P("kv", "tp", None),
        P("kv", "tp"),
        P("kv", None),
        P("kv", None),
    )
    return jax.shard_map(
        per_device,
        mesh=mesh,
        in_specs=placed,
        out_specs=(P("kv", "tp", None), P("kv", "tp", None), P("kv", "tp", None), P("kv", "tp")),
        check_vma=False,
    )
```

```python
import functools

import jax
import jax.numpy as jnp
from jax import lax
from jax.experimental import pallas as pl
from jax.experimental.pallas import tpu as pltpu
from jax.sharding import PartitionSpec as P


QB = 128
KB = 32
LIMIT = 12 << 20
F32 = jnp.float32
BF16 = jnp.bfloat16
VMEM = pl.BlockSpec(memory_space=pltpu.VMEM)
HBM = pl.BlockSpec(memory_space=pltpu.HBM)


def ring(value, by):
    count = lax.axis_size("kv")
    return lax.ppermute(value, "kv", [(i, (i + by) % count) for i in range(count)])


def swap(value, bit):
    count = lax.axis_size("kv")
    return lax.ppermute(value, "kv", [(i, i ^ bit) for i in range(count)])


def forward(msg, levels, mix):
    if levels < 4:
        return [ring(msg, -(1 << level)) for level in range(levels)]
    four = ring(msg, -4)
    eight = ring(four, -4)
    payload = mix(2, msg, four)
    two = swap(payload, 2)
    payload = mix(1, msg, two)
    one = swap(payload, 1)
    return [one, two, four, eight] + [ring(msg, -(1 << level)) for level in range(4, levels)]


def call(body, out_shape, specs, flops, nbytes, local=True):
    kept = jax.tree.map(lambda x: pltpu.VMEM(x.shape, x.dtype) if local else x, out_shape)
    return pl.pallas_call(
        body,
        out_shape=kept,
        in_specs=specs,
        out_specs=jax.tree.map(lambda _: VMEM, out_shape),
        cost_estimate=pl.CostEstimate(flops=flops, bytes_accessed=nbytes, transcendentals=0),
        compiler_params=pltpu.CompilerParams(vmem_limit_bytes=LIMIT),
    )


def nt(a, b):
    return lax.dot_general(a, b, (((1,), (1,)), ((), ())), preferred_element_type=F32)


def tn(a, b):
    return lax.dot_general(a, b, (((0,), (0,)), ((), ())), preferred_element_type=F32)


def nn(a, b):
    return lax.dot_general(a, b, (((1,), (0,)), ((), ())), preferred_element_type=F32)


PER = 8
BIG = 16384.0
LOG2E = 1.4426950408889634


def layout(tok, heads, sel):
    rows = heads * tok
    codes = 2 * rows
    stats = codes + tok // QB * sel
    return rows, codes, stats, stats + rows // 128 * PER


def thirds(row):
    high = row.astype(BF16)
    rest = row - high.astype(F32)
    middle = rest.astype(BF16)
    return high, middle, (rest - middle.astype(F32)).astype(BF16)


def pack_body(levels, heads, near, far, wanted, picked_hbm, q_hbm, g_hbm, a_hbm, lse_hbm, x_hbm, msg_ref, *refs):
    picked_ref, a_ref, lse_ref, sem, cut_sem = refs[-5:]
    rows = q_hbm.shape[0]
    tok = rows // heads
    sel = picked_ref.shape[1]
    span_blocks = tok // KB
    blocks = tok // QB
    _, codes, stats, _ = layout(tok, heads, sel)
    copies = [
        pltpu.make_async_copy(picked_hbm, picked_ref, sem.at[0]),
        pltpu.make_async_copy(lse_hbm, lse_ref, sem.at[1]),
        pltpu.make_async_copy(g_hbm, msg_ref.at[rows : 2 * rows, :], sem.at[2]),
        pltpu.make_async_copy(a_hbm, a_ref, sem.at[3]),
        pltpu.make_async_copy(q_hbm, msg_ref.at[0:rows, :], sem.at[4]),
    ]
    pieces = cuts(near, far, wanted, x_hbm, refs[:-5], cut_sem)
    for copy in copies + pieces:
        copy.start()
    me = lax.axis_index("kv")
    copies[0].wait()
    order = lax.broadcasted_iota(jnp.int32, (sel, QB), 0)
    for b in range(blocks):
        code = jnp.full((sel, QB), -1, jnp.int32)
        for p in range(sel):
            block = picked_ref[b, p]
            span = lax.div(jnp.maximum(block, 0), span_blocks)
            group = jnp.int32(0)
            for level in range(levels):
                group += ((me - span) >= (1 << level)).astype(jnp.int32)
            value = jnp.where(block < 0, -1, group * span_blocks + block - span * span_blocks)
            code = jnp.where(order == p, value, code)
        msg_ref[codes + b * sel : codes + (b + 1) * sel, :] = code.astype(F32).astype(BF16)
    copies[1].wait()
    source = lax.broadcasted_iota(jnp.int32, (tok, rows), 0)
    target = lax.broadcasted_iota(jnp.int32, (tok, rows), 1)
    logs = jnp.zeros((PER, rows), F32)
    empty = jnp.zeros((PER - 3, tok), BF16)
    for h in range(heads):
        spread = jnp.where(target == source * heads + h, 1.0, 0.0).astype(BF16)
        parts = jnp.concatenate(list(thirds(lse_ref[h : h + 1, :])) + [empty], axis=0)
        logs += nn(parts, spread)
    copies[2].wait()
    copies[3].wait()
    product = msg_ref[rows : 2 * rows, :].astype(F32) * a_ref[...].astype(F32)
    ones = jnp.ones((PER, product.shape[1]), BF16)
    dots = sum(nt(ones, part) for part in thirds(product))
    split = [part.astype(F32) for part in thirds(dots)]
    row = lax.broadcasted_iota(jnp.int32, (PER, rows), 0)
    table = jnp.where(row < 3, logs, jnp.where(row == 3, split[0], jnp.where(row == 4, split[1], split[2])))
    table = jnp.where(row < 6, table, 0.0).astype(BF16)
    for c in range(rows // 128):
        msg_ref[stats + c * PER : stats + (c + 1) * PER, :] = table[:, c * 128 : (c + 1) * 128]
    copies[4].wait()
    for copy in pieces:
        copy.wait()


def unsplit(rows):
    return (rows[0:1] + rows[1:2]) + rows[2:3]


def group_terms(msg_ref, key, value, group, heads, sel, causal):
    rows, dim = key.shape
    tok = rows // heads
    _, codes, stats, _ = layout(tok, heads, sel)
    span_blocks = tok // KB
    chunks = QB * heads // 128
    dead = [[] for _ in range(span_blocks)]
    lse, dots = [], []
    for b in range(tok // QB):
        code = msg_ref[codes + b * sel : codes + (b + 1) * sel, :].astype(F32)
        for k in range(span_blocks):
            hit = jnp.where(code == float(group * span_blocks + k), 0.0, BIG)
            dead[k] += [jnp.min(hit, axis=0, keepdims=True)] * chunks
    for c in range(rows // 128):
        stat = msg_ref[stats + c * PER : stats + (c + 1) * PER, :].astype(F32)
        lse.append(unsplit(stat[0:3]))
        dots.append(unsplit(stat[3:6]))
    lse = jnp.concatenate(lse, axis=1) * LOG2E
    dots = jnp.concatenate(dots, axis=1)
    down = lax.broadcasted_iota(jnp.int32, (8, rows), 0)
    along = lax.broadcasted_iota(jnp.int32, (8, rows), 1)
    base = jnp.where(lax.rem(down, heads) == lax.rem(along, heads), 0.0, BIG) + lse
    shift = jnp.stack([base + jnp.concatenate(dead[k], axis=1) for k in range(span_blocks)])
    query = msg_ref[0:rows, :]
    grad = msg_ref[rows : 2 * rows, :]
    scores = nt(key, query) * (dim ** (-0.5) * LOG2E)
    scores = scores.reshape(span_blocks, KB * heads // 8, 8, rows) - shift[:, None]
    scores = scores.reshape(rows, rows)
    if causal:
        key_pos = lax.broadcasted_iota(jnp.int32, (rows, rows), 0)
        query_pos = lax.broadcasted_iota(jnp.int32, (rows, rows), 1)
        scores = jnp.where(lax.div(key_pos, heads) <= lax.div(query_pos, heads), scores, -BIG)
    weights = jnp.exp2(scores)
    score_grad = weights * (nt(value, grad) - dots)
    weight_pairs = weights.astype(BF16)
    grad_pairs = score_grad.astype(BF16)
    return nn(grad_pairs, query), nn(weight_pairs, grad), tn(grad_pairs, key)


def own_body(sel, heads, msg_ref, k_ref, v_ref, dk_ref, dv_ref, dq_ref):
    dk_ref[...], dv_ref[...], dq_ref[...] = group_terms(msg_ref, k_ref[...], v_ref[...], 0, heads, sel, True)


def far_body(sel, heads, groups, last, *refs):
    count = len(groups)
    msgs = refs[:count]
    k_ref, v_ref, dk_in, dv_in = refs[count : count + 4]
    dqs = refs[count + 4 : 2 * count + 4]
    dk_out, dv_out = refs[2 * count + 4 : 2 * count + 6]
    rows, dim = k_ref.shape
    scale = dim ** (-0.5)
    dk, dv = dk_in[...], dv_in[...]
    for index, group in enumerate(groups):
        dk_term, dv_term, dq = group_terms(msgs[index], k_ref[...], v_ref[...], group, heads, sel, False)
        dk, dv = dk + dk_term, dv + dv_term
        dqs[index][...] = dq.astype(BF16)
    dv_out[...] = dv
    if not last:
        dk_out[...] = dk
        return
    round_ref = refs[-1]
    for h in range(heads):
        at = pl.ds(h, rows // heads, stride=heads) if heads > 1 else slice(None)
        round_ref[:, h * dim : (h + 1) * dim] = dv_out[at, :].astype(BF16)
    dk_out[...] = dk * scale


def query_body(dq_ref, *refs):
    out_ref = refs[-1]
    total = dq_ref[...]
    for ref in refs[:-1]:
        total = total + ref[...].astype(F32)
    out_ref[...] = total * (out_ref.shape[1] ** (-0.5))


def mix_body(bit, yes_ref, no_ref, out_ref):
    picked = (lax.axis_index("kv") & bit) != 0

    @pl.when(picked)
    def _():
        out_ref[...] = yes_ref[...]

    @pl.when(jnp.logical_not(picked))
    def _():
        out_ref[...] = no_ref[...]


def share_of(tok, m, tp):
    return tok // tp if m > 1 and tok % (16 * tp) == 0 else tok


def cuts(near, far, wanted, x_hbm, out_refs, sem):
    rank = lax.rem(lax.axis_index("kv"), near)
    width = x_hbm.shape[1] // (near * far)
    copies = []
    for index, (m, ref) in enumerate(zip(wanted, out_refs)):
        share = ref.shape[0]
        rows = slice(None)
        if share < x_hbm.shape[0]:
            rows = pl.ds(pl.multiple_of(lax.axis_index("tp") * share, share), share)
        for z in range(far):
            at = pl.multiple_of((z * near + (rank ^ m)) * width, width)
            copies.append(
                pltpu.make_async_copy(
                    x_hbm.at[rows, pl.ds(at, width)],
                    ref.at[:, z * width : (z + 1) * width],
                    sem.at[index * far + z],
                )
            )
    return copies


def cut_body(near, far, wanted, x_hbm, *refs):
    copies = cuts(near, far, wanted, x_hbm, refs[:-1], refs[-1])
    for copy in copies:
        copy.start()
    for copy in copies:
        copy.wait()


def weight_body(near, far, parity, counts, *refs):
    pieces = refs[: sum(counts)]
    rounds_refs, out_ref = refs[sum(counts) : -1], refs[-1]
    me = lax.axis_index("kv")
    depth = lax.div(me, near)
    tok = rounds_refs[0].shape[0]
    width = pieces[0].shape[1] // far
    step = 2 if parity is not None else 1
    rights = []
    for m in range(near):
        for s in range(counts[m]):
            share = tok // counts[m]
            at = lax.rem(lax.axis_index("tp") + s, counts[m]) * share if counts[m] > 1 else 0
            rights.append(rounds_refs[m][pl.ds(pl.multiple_of(at, share), share), :] if counts[m] > 1 else rounds_refs[m][...])
    right = jnp.concatenate(rights, axis=0)
    for index, rel in enumerate(range(parity or 0, far, step)):
        at = pl.multiple_of((depth ^ rel) * width, width)
        left = jnp.concatenate([piece[:, pl.ds(at, width)] for piece in pieces], axis=0)
        out_ref[index * width : (index + 1) * width, :] = tn(left, right).astype(out_ref.dtype)


def halve_body(blocks, keep_ref, came_ref, rest_ref, send_ref):
    width = keep_ref.shape[0] // blocks
    for block in range(blocks):
        at = slice(block * width, (block + 1) * width)
        to = slice(block // 2 * width, (block // 2 + 1) * width)
        total = keep_ref[at, :] + came_ref[at, :].astype(F32)
        if block % 2:
            send_ref[to, :] = total.astype(BF16)
        else:
            rest_ref[to, :] = total


def add_body(keep_ref, came_ref, out_ref):
    out_ref[...] = keep_ref[...] + came_ref[...].astype(F32)


def per_device(queries, keys, values, attended, out_grad, log_sum, picked, layer_input):
    tok, heads, dim = queries.shape
    sel = picked.shape[1]
    count = lax.axis_size("kv")
    levels = count.bit_length() - 1
    near = 1 << (levels // 2)
    far = count // near
    tp = lax.axis_size("tp")
    rows, _, _, msg_rows = layout(tok, heads, sel)
    flat = lambda x: x.reshape(rows, dim)
    key, value = flat(keys), flat(values)

    def shape(dims, kind):
        return jax.ShapeDtypeStruct(dims, kind)

    pairs = rows * rows * dim * 10
    width = layer_input.shape[1] // count
    blocked = width % 128 == 0 and far > 1
    shares = [share_of(tok, m, tp) for m in range(near)]
    early = list(range(2, near)) if blocked else []
    msg, *first = pl.pallas_call(
        functools.partial(pack_body, levels, heads, near, far, early),
        out_shape=[pltpu.VMEM((msg_rows, dim), BF16)]
        + [pltpu.VMEM((shares[m], far * width), BF16) for m in early],
        in_specs=[HBM] * 6,
        out_specs=[VMEM] * (1 + len(early)),
        scratch_shapes=[
            pltpu.SMEM(picked.shape, jnp.int32),
            pltpu.VMEM((rows, dim), BF16),
            pltpu.VMEM((heads, tok), F32),
            pltpu.SemaphoreType.DMA((5,)),
            pltpu.SemaphoreType.DMA((max(1, len(early)) * far,)),
        ],
        compiler_params=pltpu.CompilerParams(vmem_limit_bytes=62000000),
    )(picked, flat(queries), flat(out_grad), flat(attended), log_sum.T, layer_input)

    def mix(bit, yes, no):
        return call(
            functools.partial(mix_body, bit), shape(yes.shape, BF16), [VMEM, VMEM], 1 << 18, yes.size * 6
        )(yes, no)

    got = forward(msg, levels, mix)
    if blocked:
        wanted = [m for m in (1, 0) if m < near]
        later = pl.pallas_call(
            functools.partial(cut_body, near, far, wanted),
            out_shape=[pltpu.VMEM((tok, far * width), BF16) for _ in wanted],
            in_specs=[HBM],
            out_specs=[VMEM] * len(wanted),
            scratch_shapes=[pltpu.SemaphoreType.DMA((len(wanted) * far,))],
            cost_estimate=pl.CostEstimate(flops=1 << 20, bytes_accessed=layer_input.size, transcendentals=0),
            compiler_params=pltpu.CompilerParams(vmem_limit_bytes=56 << 20),
        )(layer_input)
        cut = dict(zip(early + wanted, first + list(later)))
        pieces, counts = [cut[0]], [1]
        for m in range(1, near):
            pieces.append(swap(cut[m], m))
            counts.append(tok // shares[m])
            first = pieces[-1]
            for s in range(1, counts[m]):
                pieces.append(lax.ppermute(first, "tp", [((i + s) % tp, i) for i in range(tp)]))
    dk_own, dv_own, dq_own = call(
        functools.partial(own_body, sel, heads),
        [shape((rows, dim), F32)] * 3,
        [VMEM] * 3,
        pairs, 8 * rows * dim * 4,
    )(msg, key, value)

    def far_call(groups, dk, dv, last):
        kinds = [shape((rows, dim), BF16)] * len(groups) + [shape((rows, dim), F32)] * 2
        if last:
            kinds.append(shape((tok, heads * dim), BF16))
        return call(
            functools.partial(far_body, sel, heads, groups, last),
            kinds,
            [VMEM] * (len(groups) + 4),
            pairs * len(groups), 8 * rows * dim,
        )(*[got[group - 1] for group in groups], key, value, dk, dv)

    back, dk, dv = {}, dk_own, dv_own
    stages = [(3,), (2,), (4,), (1,)] + [(level,) for level in range(5, levels + 1)]
    if levels < 4:
        stages = [tuple(range(1, levels + 1))]
    elif levels > 4:
        stages = [(level,) for level in range(1, levels + 1)]
    for stage in stages:
        outs = far_call(stage, dk, dv, stage == stages[-1])
        for group, side in zip(stage, outs):
            back[group] = ring(side, 1 << (group - 1))
        outs = outs[len(stage) :]
        dk, dv = outs[:2]
    key_grad, value_grad, rounded = outs
    if blocked:
        rounds = {0: rounded}
        bit = near // 2
        while bit:
            for m in list(rounds):
                rounds[m ^ bit] = swap(rounds[m], bit)
            bit //= 2
        columns = heads * dim

        def weight(parity, kind):
            blocks = far // 2
            return call(
                functools.partial(weight_body, near, far, parity, counts),
                shape((blocks * width, columns), kind),
                [VMEM] * (len(pieces) + near),
                2 * near * tok * blocks * width * columns, near * tok * far * width * 2,
            )(*pieces, *[rounds[m] for m in range(near)])

        send = weight(1, BF16)
        total = weight(0, F32)
        bit, left = near, far // 2
        came = swap(send, bit)
        while left > 1:
            bit *= 2
            total, send = call(
                functools.partial(halve_body, left),
                [shape((left // 2 * width, columns), F32), shape((left // 2 * width, columns), BF16)],
                [VMEM] * 2, 1 << 18, left * width * columns * 8,
            )(total, came)
            left //= 2
            came = swap(send, bit)
        total = call(add_body, shape(total.shape, F32), [VMEM] * 2, 1 << 18, total.size * 10, False)(total, came)
    else:
        terms = lax.dot_general(
            layer_input, rounded, (((0,), (0,)), ((), ())), preferred_element_type=F32
        )
        total = lax.psum_scatter(terms, "kv", scatter_dimension=0, tiled=True)
    query_grad = call(
        query_body, shape((rows, dim), F32), [VMEM] * (levels + 1), 1 << 20, rows * dim * 16, False
    )(dq_own, *[back[group] for group in range(1, levels + 1)])
    grads = [x.reshape(tok, heads, dim) for x in (query_grad, key_grad, value_grad)]
    return (*grads, total)


def solution(mesh):
    placed = (
        P("kv", "tp", None),
        P("kv", "tp", None),
        P("kv", "tp", None),
        P("kv", "tp", None),
        P("kv", "tp", None),
        P("kv", "tp"),
        P("kv", None),
        P("kv", None),
    )
    return jax.shard_map(
        per_device,
        mesh=mesh,
        in_specs=placed,
        out_specs=(P("kv", "tp", None), P("kv", "tp", None), P("kv", "tp", None), P("kv", "tp")),
        check_vma=False,
    )
```

```python
import functools

import jax
import jax.numpy as jnp
from jax import lax
from jax.experimental import pallas as pl
from jax.experimental.pallas import tpu as pltpu
from jax.sharding import PartitionSpec as P


QB = 128
KB = 32
LIMIT = 12 << 20
F32 = jnp.float32
BF16 = jnp.bfloat16
VMEM = pl.BlockSpec(memory_space=pltpu.VMEM)
HBM = pl.BlockSpec(memory_space=pltpu.HBM)


def ring(value, by):
    count = lax.axis_size("kv")
    return lax.ppermute(value, "kv", [(i, (i + by) % count) for i in range(count)])


def line(value, by):
    count = lax.axis_size("kv")
    return lax.ppermute(value, "kv", [(i, i + by) for i in range(count) if 0 <= i + by < count])


def swap(value, bit):
    count = lax.axis_size("kv")
    return lax.ppermute(value, "kv", [(i, i ^ bit) for i in range(count)])


def forward(msg, levels, mix):
    if levels < 4:
        return [ring(msg, -(1 << level)) for level in range(levels)]
    four = line(msg, -4)
    eight = ring(four, -4)
    payload = mix(2, msg, four)
    two = swap(payload, 2)
    payload = mix(1, msg, two)
    one = swap(payload, 1)
    return [one, two, four, eight] + [ring(msg, -(1 << level)) for level in range(4, levels)]


def call(body, out_shape, specs, flops, nbytes, local=True):
    kept = jax.tree.map(lambda x: pltpu.VMEM(x.shape, x.dtype) if local else x, out_shape)
    return pl.pallas_call(
        body,
        out_shape=kept,
        in_specs=specs,
        out_specs=jax.tree.map(lambda _: VMEM, out_shape),
        cost_estimate=pl.CostEstimate(flops=flops, bytes_accessed=nbytes, transcendentals=0),
        compiler_params=pltpu.CompilerParams(vmem_limit_bytes=LIMIT),
    )


def nt(a, b):
    return lax.dot_general(a, b, (((1,), (1,)), ((), ())), preferred_element_type=F32)


def tn(a, b):
    return lax.dot_general(a, b, (((0,), (0,)), ((), ())), preferred_element_type=F32)


def nn(a, b):
    return lax.dot_general(a, b, (((1,), (0,)), ((), ())), preferred_element_type=F32)


PER = 8
BIG = 16384.0
LOG2E = 1.4426950408889634


def layout(tok, heads, sel):
    rows = heads * tok
    codes = 2 * rows
    stats = codes + tok // QB * sel
    return rows, codes, stats, stats + rows // 128 * PER


def thirds(row):
    high = row.astype(BF16)
    rest = row - high.astype(F32)
    middle = rest.astype(BF16)
    return high, middle, (rest - middle.astype(F32)).astype(BF16)


def pack_body(levels, heads, near, far, wanted, picked_hbm, q_hbm, g_hbm, a_hbm, lse_hbm, x_hbm, k_hbm, v_hbm, msg_ref, *refs):
    picked_ref, a_ref, lse_ref, sem, cut_sem = refs[-5:]
    rows = q_hbm.shape[0]
    tok = rows // heads
    sel = picked_ref.shape[1]
    span_blocks = tok // KB
    blocks = tok // QB
    _, codes, stats, _ = layout(tok, heads, sel)
    copies = [
        pltpu.make_async_copy(picked_hbm, picked_ref, sem.at[0]),
        pltpu.make_async_copy(lse_hbm, lse_ref, sem.at[1]),
        pltpu.make_async_copy(g_hbm, msg_ref.at[rows : 2 * rows, :], sem.at[2]),
        pltpu.make_async_copy(a_hbm, a_ref, sem.at[3]),
        pltpu.make_async_copy(q_hbm, msg_ref.at[0:rows, :], sem.at[4]),
    ]
    kv_ref = refs[0]
    pieces = cuts(near, far, wanted, x_hbm, refs[1:-5], cut_sem)
    pieces += [
        pltpu.make_async_copy(k_hbm, kv_ref.at[0:rows, :], sem.at[5]),
        pltpu.make_async_copy(v_hbm, kv_ref.at[rows : 2 * rows, :], sem.at[6]),
    ]
    for copy in copies + pieces:
        copy.start()
    me = lax.axis_index("kv")
    copies[0].wait()
    order = lax.broadcasted_iota(jnp.int32, (sel, QB), 0)
    for b in range(blocks):
        code = jnp.full((sel, QB), -1, jnp.int32)
        for p in range(sel):
            block = picked_ref[b, p]
            span = lax.div(jnp.maximum(block, 0), span_blocks)
            group = jnp.int32(0)
            for level in range(levels):
                group += ((me - span) >= (1 << level)).astype(jnp.int32)
            value = jnp.where(block < 0, -1, group * span_blocks + block - span * span_blocks)
            code = jnp.where(order == p, value, code)
        msg_ref[codes + b * sel : codes + (b + 1) * sel, :] = code.astype(F32).astype(BF16)
    copies[1].wait()
    source = lax.broadcasted_iota(jnp.int32, (tok, rows), 0)
    target = lax.broadcasted_iota(jnp.int32, (tok, rows), 1)
    logs = jnp.zeros((PER, rows), F32)
    empty = jnp.zeros((PER - 3, tok), BF16)
    for h in range(heads):
        spread = jnp.where(target == source * heads + h, 1.0, 0.0).astype(BF16)
        parts = jnp.concatenate(list(thirds(lse_ref[h : h + 1, :])) + [empty], axis=0)
        logs += nn(parts, spread)
    copies[2].wait()
    copies[3].wait()
    product = msg_ref[rows : 2 * rows, :].astype(F32) * a_ref[...].astype(F32)
    ones = jnp.ones((PER, product.shape[1]), BF16)
    dots = sum(nt(ones, part) for part in thirds(product))
    split = [part.astype(F32) for part in thirds(dots)]
    row = lax.broadcasted_iota(jnp.int32, (PER, rows), 0)
    table = jnp.where(row < 3, logs, jnp.where(row == 3, split[0], jnp.where(row == 4, split[1], split[2])))
    table = jnp.where(row < 6, table, 0.0).astype(BF16)
    for c in range(rows // 128):
        msg_ref[stats + c * PER : stats + (c + 1) * PER, :] = table[:, c * 128 : (c + 1) * 128]
    copies[4].wait()
    for copy in pieces:
        copy.wait()


def unsplit(rows):
    return (rows[0:1] + rows[1:2]) + rows[2:3]


def group_terms(msg_ref, key, value, group, heads, sel, causal, grads=True, side=True):
    rows, dim = key.shape
    tok = rows // heads
    _, codes, stats, _ = layout(tok, heads, sel)
    span_blocks = tok // KB
    chunks = QB * heads // 128
    dead = [[] for _ in range(span_blocks)]
    lse, dots = [], []
    for b in range(tok // QB):
        code = msg_ref[codes + b * sel : codes + (b + 1) * sel, :].astype(F32)
        for k in range(span_blocks):
            hit = jnp.where(code == float(group * span_blocks + k), 0.0, BIG)
            dead[k] += [jnp.min(hit, axis=0, keepdims=True)] * chunks
    for c in range(rows // 128):
        stat = msg_ref[stats + c * PER : stats + (c + 1) * PER, :].astype(F32)
        lse.append(unsplit(stat[0:3]))
        dots.append(unsplit(stat[3:6]))
    lse = jnp.concatenate(lse, axis=1) * LOG2E
    dots = jnp.concatenate(dots, axis=1)
    down = lax.broadcasted_iota(jnp.int32, (8, rows), 0)
    along = lax.broadcasted_iota(jnp.int32, (8, rows), 1)
    base = jnp.where(lax.rem(down, heads) == lax.rem(along, heads), 0.0, BIG) + lse
    shift = jnp.stack([base + jnp.concatenate(dead[k], axis=1) for k in range(span_blocks)])
    query = msg_ref[0:rows, :]
    grad = msg_ref[rows : 2 * rows, :]
    scores = nt(key, query) * (dim ** (-0.5) * LOG2E)
    scores = scores.reshape(span_blocks, KB * heads // 8, 8, rows) - shift[:, None]
    scores = scores.reshape(rows, rows)
    if causal:
        key_pos = lax.broadcasted_iota(jnp.int32, (rows, rows), 0)
        query_pos = lax.broadcasted_iota(jnp.int32, (rows, rows), 1)
        scores = jnp.where(lax.div(key_pos, heads) <= lax.div(query_pos, heads), scores, -BIG)
    weights = jnp.exp2(scores)
    score_grad = weights * (nt(value, grad) - dots)
    weight_pairs = weights.astype(BF16)
    grad_pairs = score_grad.astype(BF16)
    query_term = tn(grad_pairs, key) if side else None
    if not grads:
        return query_term
    return nn(grad_pairs, query), nn(weight_pairs, grad), query_term


def near_body(sel, heads, group, msg_ref, kv_ref, dq_in, dq_out):
    rows = kv_ref.shape[0] // 2
    term = group_terms(msg_ref, kv_ref[0:rows, :], kv_ref[rows : 2 * rows, :], group, heads, sel, False, False)
    dq_out[...] = dq_in[...] + term


def own_body(sel, heads, msg_ref, k_ref, v_ref, dk_ref, dv_ref, dq_ref):
    dk_ref[...], dv_ref[...], dq_ref[...] = group_terms(msg_ref, k_ref[...], v_ref[...], 0, heads, sel, True)


def far_body(sel, heads, groups, last, sides, *refs):
    count = len(groups)
    msgs = refs[:count]
    k_ref, v_ref, dk_in, dv_in = refs[count : count + 4]
    dqs = refs[count + 4 : count + 4 + len(sides)]
    dk_out, dv_out = refs[count + 4 + len(sides) : count + 6 + len(sides)]
    rows, dim = k_ref.shape
    scale = dim ** (-0.5)
    dk, dv = dk_in[...], dv_in[...]
    for index, group in enumerate(groups):
        dk_term, dv_term, dq = group_terms(
            msgs[index], k_ref[...], v_ref[...], group, heads, sel, False, True, group in sides
        )
        dk, dv = dk + dk_term, dv + dv_term
        if group in sides:
            dqs[sides.index(group)][...] = dq.astype(BF16)
    dv_out[...] = dv
    if not last:
        dk_out[...] = dk
        return
    round_ref = refs[-1]
    for h in range(heads):
        at = pl.ds(h, rows // heads, stride=heads) if heads > 1 else slice(None)
        round_ref[:, h * dim : (h + 1) * dim] = dv_out[at, :].astype(BF16)
    dk_out[...] = dk * scale


def query_body(dq_ref, *refs):
    out_ref = refs[-1]
    total = dq_ref[...]
    for ref in refs[:-1]:
        total = total + ref[...].astype(F32)
    out_ref[...] = total * (out_ref.shape[1] ** (-0.5))


def mix_body(bit, yes_ref, no_ref, out_ref):
    picked = (lax.axis_index("kv") & bit) != 0

    @pl.when(picked)
    def _():
        out_ref[...] = yes_ref[...]

    @pl.when(jnp.logical_not(picked))
    def _():
        out_ref[...] = no_ref[...]


def shares_of(tok, m, near, tp):
    share = tok // tp
    if m < 2 or share % 32:
        return [(0, tok)]
    if m < near - 1:
        return [(0, share)]
    return [(0, share // 2), (share // 2, share // 2)]


def cuts(near, far, wanted, x_hbm, out_refs, sem):
    rank = lax.rem(lax.axis_index("kv"), near)
    width = x_hbm.shape[1] // (near * far)
    copies = []
    for index, ((m, first, share), ref) in enumerate(zip(wanted, out_refs)):
        rows = slice(None)
        if share < x_hbm.shape[0]:
            of_plane = x_hbm.shape[0] // lax.axis_size("tp")
            rows = pl.ds(pl.multiple_of(lax.axis_index("tp") * of_plane + first, share), share)
        for z in range(far):
            at = pl.multiple_of((z * near + (rank ^ m)) * width, width)
            copies.append(
                pltpu.make_async_copy(
                    x_hbm.at[rows, pl.ds(at, width)],
                    ref.at[:, z * width : (z + 1) * width],
                    sem.at[index * far + z],
                )
            )
    return copies


def cut_body(near, far, wanted, x_hbm, *refs):
    copies = cuts(near, far, wanted, x_hbm, refs[:-1], refs[-1])
    for copy in copies:
        copy.start()
    for copy in copies:
        copy.wait()


def weight_body(near, far, parity, plan, *refs):
    pieces = refs[: len(plan)]
    rounds_refs, out_ref = refs[len(plan) : -1], refs[-1]
    depth = lax.div(lax.axis_index("kv"), near)
    tok = rounds_refs[0].shape[0]
    width = pieces[0].shape[1] // far
    rights = []
    for m, first, share, turn in plan:
        if share == tok:
            rights.append(rounds_refs[m][...])
            continue
        planes = lax.axis_size("tp")
        at = lax.rem(lax.axis_index("tp") + turn, planes) * (tok // planes) + first
        rights.append(rounds_refs[m][pl.ds(pl.multiple_of(at, share), share), :])
    right = jnp.concatenate(rights, axis=0)
    for index, rel in enumerate(range(parity, far, 2)):
        at = pl.multiple_of((depth ^ rel) * width, width)
        left = jnp.concatenate([piece[:, pl.ds(at, width)] for piece in pieces], axis=0)
        out_ref[index * width : (index + 1) * width, :] = tn(left, right).astype(out_ref.dtype)


def halve_body(blocks, keep_ref, came_ref, rest_ref, send_ref):
    width = keep_ref.shape[0] // blocks
    for block in range(blocks):
        at = slice(block * width, (block + 1) * width)
        to = slice(block // 2 * width, (block // 2 + 1) * width)
        total = keep_ref[at, :] + came_ref[at, :].astype(F32)
        if block % 2:
            send_ref[to, :] = total.astype(BF16)
        else:
            rest_ref[to, :] = total


def add_body(keep_ref, came_ref, out_ref):
    out_ref[...] = keep_ref[...] + came_ref[...].astype(F32)


def per_device(queries, keys, values, attended, out_grad, log_sum, picked, layer_input):
    tok, heads, dim = queries.shape
    sel = picked.shape[1]
    count = lax.axis_size("kv")
    levels = count.bit_length() - 1
    near = 1 << (levels // 2)
    far = count // near
    tp = lax.axis_size("tp")
    rows, _, _, msg_rows = layout(tok, heads, sel)
    flat = lambda x: x.reshape(rows, dim)
    key, value = flat(keys), flat(values)

    def shape(dims, kind):
        return jax.ShapeDtypeStruct(dims, kind)

    pairs = rows * rows * dim * 10
    width = layer_input.shape[1] // count
    blocked = width % 128 == 0 and far > 1
    early = []
    if blocked:
        early = [(m, *part) for m in range(2, near) for part in shares_of(tok, m, near, tp)]
    msg, kv, *first = pl.pallas_call(
        functools.partial(pack_body, levels, heads, near, far, early),
        out_shape=[pltpu.VMEM((msg_rows, dim), BF16), pltpu.VMEM((2 * rows, dim), BF16)]
        + [pltpu.VMEM((part[2], far * width), BF16) for part in early],
        in_specs=[HBM] * 8,
        out_specs=[VMEM] * (2 + len(early)),
        scratch_shapes=[
            pltpu.SMEM(picked.shape, jnp.int32),
            pltpu.VMEM((rows, dim), BF16),
            pltpu.VMEM((heads, tok), F32),
            pltpu.SemaphoreType.DMA((7,)),
            pltpu.SemaphoreType.DMA((max(1, len(early)) * far,)),
        ],
        compiler_params=pltpu.CompilerParams(vmem_limit_bytes=62000000),
    )(picked, flat(queries), flat(out_grad), flat(attended), log_sum.T, layer_input, key, value)
    far_kv = line(kv, 1 << (levels - 1))

    def mix(bit, yes, no):
        return call(
            functools.partial(mix_body, bit), shape(yes.shape, BF16), [VMEM, VMEM], 1 << 18, yes.size * 6
        )(yes, no)

    got = forward(msg, levels, mix)
    if blocked:
        wanted = [(m, 0, tok) for m in (1, 0) if m < near]
        later = pl.pallas_call(
            functools.partial(cut_body, near, far, wanted),
            out_shape=[pltpu.VMEM((tok, far * width), BF16) for _ in wanted],
            in_specs=[HBM],
            out_specs=[VMEM] * len(wanted),
            scratch_shapes=[pltpu.SemaphoreType.DMA((len(wanted) * far,))],
            cost_estimate=pl.CostEstimate(flops=1 << 20, bytes_accessed=layer_input.size, transcendentals=0),
            compiler_params=pltpu.CompilerParams(vmem_limit_bytes=56 << 20),
        )(layer_input)
        cut = dict(zip(early + wanted, first + list(later)))
        pieces, plan = [], []
        for (m, start, share), piece in cut.items():
            if m:
                piece = swap(piece, m)
            pieces.append(piece)
            plan.append((m, start, share, 0))
            if share == tok:
                continue
            for s in range(1, tp):
                pieces.append(lax.ppermute(piece, "tp", [((i + s) % tp, i) for i in range(tp)]))
                plan.append((m, start, share, s))
    dk_own, dv_own, dq_own = call(
        functools.partial(own_body, sel, heads),
        [shape((rows, dim), F32)] * 3,
        [VMEM] * 3,
        pairs, 8 * rows * dim * 4,
    )(msg, key, value)

    dq_near = call(
        functools.partial(near_body, sel, heads, levels),
        shape((rows, dim), F32), [VMEM] * 3, pairs * 3 // 5, 8 * rows * dim,
    )(msg, far_kv, dq_own)

    def far_call(groups, dk, dv, last):
        sides = [group for group in groups if group != levels]
        kinds = [shape((rows, dim), BF16)] * len(sides) + [shape((rows, dim), F32)] * 2
        if last:
            kinds.append(shape((tok, heads * dim), BF16))
        return call(
            functools.partial(far_body, sel, heads, groups, last, sides),
            kinds,
            [VMEM] * (len(groups) + 4),
            pairs * len(groups), 8 * rows * dim,
        )(*[got[group - 1] for group in groups], key, value, dk, dv)

    back, dk, dv = {}, dk_own, dv_own
    stages = [(3,), (2,), (4,), (1,)] + [(level,) for level in range(5, levels + 1)]
    if levels < 4:
        stages = [tuple(range(1, levels + 1))]
    elif levels > 4:
        stages = [(level,) for level in range(1, levels + 1)]
    for stage in stages:
        outs = far_call(stage, dk, dv, stage == stages[-1])
        sides = [group for group in stage if group != levels]
        for group, side in zip(sides, outs):
            back[group] = ring(side, 1 << (group - 1))
        outs = outs[len(sides) :]
        dk, dv = outs[:2]
    key_grad, value_grad, rounded = outs
    if blocked:
        rounds = {0: rounded}
        bit = near // 2
        while bit:
            for m in list(rounds):
                rounds[m ^ bit] = swap(rounds[m], bit)
            bit //= 2
        columns = heads * dim

        def weight(parity, kind):
            blocks = far // 2
            return call(
                functools.partial(weight_body, near, far, parity, plan),
                shape((blocks * width, columns), kind),
                [VMEM] * (len(pieces) + near),
                2 * near * tok * blocks * width * columns, near * tok * far * width * 2,
            )(*pieces, *[rounds[m] for m in range(near)])

        send = weight(1, BF16)
        total = weight(0, F32)
        bit, left = near, far // 2
        came = swap(send, bit)
        while left > 1:
            bit *= 2
            total, send = call(
                functools.partial(halve_body, left),
                [shape((left // 2 * width, columns), F32), shape((left // 2 * width, columns), BF16)],
                [VMEM] * 2, 1 << 18, left * width * columns * 8,
            )(total, came)
            left //= 2
            came = swap(send, bit)
        total = call(add_body, shape(total.shape, F32), [VMEM] * 2, 1 << 18, total.size * 10, False)(total, came)
    else:
        terms = lax.dot_general(
            layer_input, rounded, (((0,), (0,)), ((), ())), preferred_element_type=F32
        )
        total = lax.psum_scatter(terms, "kv", scatter_dimension=0, tiled=True)
    query_grad = call(
        query_body, shape((rows, dim), F32), [VMEM] * levels, 1 << 20, rows * dim * 16, False
    )(dq_near, *[back[group] for group in range(1, levels)])
    grads = [x.reshape(tok, heads, dim) for x in (query_grad, key_grad, value_grad)]
    return (*grads, total)


def solution(mesh):
    placed = (
        P("kv", "tp", None),
        P("kv", "tp", None),
        P("kv", "tp", None),
        P("kv", "tp", None),
        P("kv", "tp", None),
        P("kv", "tp"),
        P("kv", None),
        P("kv", None),
    )
    return jax.shard_map(
        per_device,
        mesh=mesh,
        in_specs=placed,
        out_specs=(P("kv", "tp", None), P("kv", "tp", None), P("kv", "tp", None), P("kv", "tp")),
        check_vma=False,
    )
```

```python
import functools

import jax
import jax.numpy as jnp
from jax import lax
from jax.experimental import pallas as pl
from jax.experimental.pallas import tpu as pltpu
from jax.sharding import PartitionSpec as P


QB = 128
KB = 32
LIMIT = 12 << 20
F32 = jnp.float32
BF16 = jnp.bfloat16
VMEM = pl.BlockSpec(memory_space=pltpu.VMEM)
HBM = pl.BlockSpec(memory_space=pltpu.HBM)


def ring(value, by):
    count = lax.axis_size("kv")
    return lax.ppermute(value, "kv", [(i, (i + by) % count) for i in range(count)])


def line(value, by):
    count = lax.axis_size("kv")
    return lax.ppermute(value, "kv", [(i, i + by) for i in range(count) if 0 <= i + by < count])


def swap(value, bit):
    count = lax.axis_size("kv")
    return lax.ppermute(value, "kv", [(i, i ^ bit) for i in range(count)])


def forward(msg, levels, mix):
    if levels < 4:
        return [ring(msg, -(1 << level)) for level in range(levels)]
    four = line(msg, -4)
    eight = ring(four, -4)
    payload = mix(2, msg, four)
    two = swap(payload, 2)
    payload = mix(1, msg, two)
    one = swap(payload, 1)
    return [one, two, four, eight] + [ring(msg, -(1 << level)) for level in range(4, levels)]


def call(body, out_shape, specs, flops, nbytes, local=True):
    kept = jax.tree.map(lambda x: pltpu.VMEM(x.shape, x.dtype) if local else x, out_shape)
    return pl.pallas_call(
        body,
        out_shape=kept,
        in_specs=specs,
        out_specs=jax.tree.map(lambda _: VMEM, out_shape),
        cost_estimate=pl.CostEstimate(flops=flops, bytes_accessed=nbytes, transcendentals=0),
        compiler_params=pltpu.CompilerParams(vmem_limit_bytes=LIMIT),
    )


def nt(a, b):
    return lax.dot_general(a, b, (((1,), (1,)), ((), ())), preferred_element_type=F32)


def tn(a, b):
    return lax.dot_general(a, b, (((0,), (0,)), ((), ())), preferred_element_type=F32)


def nn(a, b):
    return lax.dot_general(a, b, (((1,), (0,)), ((), ())), preferred_element_type=F32)


PER = 8
BIG = 16384.0
LOG2E = 1.4426950408889634


def layout(tok, heads, sel):
    rows = heads * tok
    codes = 2 * rows
    stats = codes + tok // QB * sel
    return rows, codes, stats, stats + rows // 128 * PER


def thirds(row):
    high = row.astype(BF16)
    rest = row - high.astype(F32)
    middle = rest.astype(BF16)
    return high, middle, (rest - middle.astype(F32)).astype(BF16)


def pack_body(levels, heads, near, far, wanted, picked_hbm, q_hbm, g_hbm, a_hbm, lse_hbm, x_hbm, k_hbm, v_hbm, msg_ref, *refs):
    picked_ref, a_ref, lse_ref, sem, cut_sem = refs[-5:]
    rows = q_hbm.shape[0]
    tok = rows // heads
    sel = picked_ref.shape[1]
    span_blocks = tok // KB
    blocks = tok // QB
    _, codes, stats, _ = layout(tok, heads, sel)
    copies = [
        pltpu.make_async_copy(picked_hbm, picked_ref, sem.at[0]),
        pltpu.make_async_copy(lse_hbm, lse_ref, sem.at[1]),
        pltpu.make_async_copy(g_hbm, msg_ref.at[rows : 2 * rows, :], sem.at[2]),
        pltpu.make_async_copy(a_hbm, a_ref, sem.at[3]),
        pltpu.make_async_copy(q_hbm, msg_ref.at[0:rows, :], sem.at[4]),
    ]
    kv_ref = refs[0]
    pieces = cuts(near, far, wanted, x_hbm, refs[1:-5], cut_sem)
    pieces += [
        pltpu.make_async_copy(k_hbm, kv_ref.at[0:rows, :], sem.at[5]),
        pltpu.make_async_copy(v_hbm, kv_ref.at[rows : 2 * rows, :], sem.at[6]),
    ]
    for copy in copies + pieces:
        copy.start()
    me = lax.axis_index("kv")
    copies[0].wait()
    order = lax.broadcasted_iota(jnp.int32, (sel, QB), 0)
    for b in range(blocks):
        code = jnp.full((sel, QB), -1, jnp.int32)
        for p in range(sel):
            block = picked_ref[b, p]
            span = lax.div(jnp.maximum(block, 0), span_blocks)
            group = jnp.int32(0)
            for level in range(levels):
                group += ((me - span) >= (1 << level)).astype(jnp.int32)
            value = jnp.where(block < 0, -1, group * span_blocks + block - span * span_blocks)
            code = jnp.where(order == p, value, code)
        msg_ref[codes + b * sel : codes + (b + 1) * sel, :] = code.astype(F32).astype(BF16)
    copies[1].wait()
    source = lax.broadcasted_iota(jnp.int32, (tok, rows), 0)
    target = lax.broadcasted_iota(jnp.int32, (tok, rows), 1)
    logs = jnp.zeros((PER, rows), F32)
    empty = jnp.zeros((PER - 3, tok), BF16)
    for h in range(heads):
        spread = jnp.where(target == source * heads + h, 1.0, 0.0).astype(BF16)
        parts = jnp.concatenate(list(thirds(lse_ref[h : h + 1, :])) + [empty], axis=0)
        logs += nn(parts, spread)
    copies[2].wait()
    copies[3].wait()
    product = msg_ref[rows : 2 * rows, :].astype(F32) * a_ref[...].astype(F32)
    ones = jnp.ones((PER, product.shape[1]), BF16)
    dots = sum(nt(ones, part) for part in thirds(product))
    split = [part.astype(F32) for part in thirds(dots)]
    row = lax.broadcasted_iota(jnp.int32, (PER, rows), 0)
    table = jnp.where(row < 3, logs, jnp.where(row == 3, split[0], jnp.where(row == 4, split[1], split[2])))
    table = jnp.where(row < 6, table, 0.0).astype(BF16)
    for c in range(rows // 128):
        msg_ref[stats + c * PER : stats + (c + 1) * PER, :] = table[:, c * 128 : (c + 1) * 128]
    copies[4].wait()
    for copy in pieces:
        copy.wait()


def unsplit(rows):
    return (rows[0:1] + rows[1:2]) + rows[2:3]


def group_terms(msg_ref, key, value, group, heads, sel, causal, grads=True, side=True):
    rows, dim = key.shape
    tok = rows // heads
    _, codes, stats, _ = layout(tok, heads, sel)
    span_blocks = tok // KB
    chunks = QB * heads // 128
    dead = [[] for _ in range(span_blocks)]
    lse, dots = [], []
    for b in range(tok // QB):
        code = msg_ref[codes + b * sel : codes + (b + 1) * sel, :].astype(F32)
        for k in range(span_blocks):
            hit = jnp.where(code == float(group * span_blocks + k), 0.0, BIG)
            dead[k] += [jnp.min(hit, axis=0, keepdims=True)] * chunks
    for c in range(rows // 128):
        stat = msg_ref[stats + c * PER : stats + (c + 1) * PER, :].astype(F32)
        lse.append(unsplit(stat[0:3]))
        dots.append(unsplit(stat[3:6]))
    lse = jnp.concatenate(lse, axis=1) * LOG2E
    dots = jnp.concatenate(dots, axis=1)
    down = lax.broadcasted_iota(jnp.int32, (8, rows), 0)
    along = lax.broadcasted_iota(jnp.int32, (8, rows), 1)
    base = jnp.where(lax.rem(down, heads) == lax.rem(along, heads), 0.0, BIG) + lse
    shift = jnp.stack([base + jnp.concatenate(dead[k], axis=1) for k in range(span_blocks)])
    query = msg_ref[0:rows, :]
    grad = msg_ref[rows : 2 * rows, :]
    scores = nt(key, query) * (dim ** (-0.5) * LOG2E)
    scores = scores.reshape(span_blocks, KB * heads // 8, 8, rows) - shift[:, None]
    scores = scores.reshape(rows, rows)
    if causal:
        key_pos = lax.broadcasted_iota(jnp.int32, (rows, rows), 0)
        query_pos = lax.broadcasted_iota(jnp.int32, (rows, rows), 1)
        scores = jnp.where(lax.div(key_pos, heads) <= lax.div(query_pos, heads), scores, -BIG)
    weights = jnp.exp2(scores)
    score_grad = weights * (nt(value, grad) - dots)
    weight_pairs = weights.astype(BF16)
    grad_pairs = score_grad.astype(BF16)
    query_term = tn(grad_pairs, key) if side else None
    if not grads:
        return query_term
    return nn(grad_pairs, query), nn(weight_pairs, grad), query_term


def near_body(sel, heads, group, msg_ref, kv_ref, dq_in, dq_out):
    rows = kv_ref.shape[0] // 2
    term = group_terms(msg_ref, kv_ref[0:rows, :], kv_ref[rows : 2 * rows, :], group, heads, sel, False, False)
    dq_out[...] = dq_in[...] + term


def own_body(sel, heads, msg_ref, kv_ref, dk_ref, dv_ref, dq_ref):
    rows = kv_ref.shape[0] // 2
    k_ref, v_ref = kv_ref.at[0:rows, :], kv_ref.at[rows : 2 * rows, :]
    dk_ref[...], dv_ref[...], dq_ref[...] = group_terms(msg_ref, k_ref[...], v_ref[...], 0, heads, sel, True)


def far_body(sel, heads, groups, last, sides, *refs):
    count = len(groups)
    msgs = refs[:count]
    kv_ref, dk_in, dv_in = refs[count : count + 3]
    rows = kv_ref.shape[0] // 2
    k_ref, v_ref = kv_ref.at[0:rows, :], kv_ref.at[rows : 2 * rows, :]
    dqs = refs[count + 3 : count + 3 + len(sides)]
    dk_out, dv_out = refs[count + 3 + len(sides) : count + 5 + len(sides)]
    dim = kv_ref.shape[1]
    scale = dim ** (-0.5)
    dk, dv = dk_in[...], dv_in[...]
    for index, group in enumerate(groups):
        dk_term, dv_term, dq = group_terms(
            msgs[index], k_ref[...], v_ref[...], group, heads, sel, False, True, group in sides
        )
        dk, dv = dk + dk_term, dv + dv_term
        if group in sides:
            dqs[sides.index(group)][...] = dq.astype(BF16)
    dv_out[...] = dv
    if not last:
        dk_out[...] = dk
        return
    round_ref = refs[-1]
    for h in range(heads):
        at = pl.ds(h, rows // heads, stride=heads) if heads > 1 else slice(None)
        round_ref[:, h * dim : (h + 1) * dim] = dv_out[at, :].astype(BF16)
    dk_out[...] = dk * scale


def query_body(dq_ref, *refs):
    out_ref = refs[-1]
    total = dq_ref[...]
    for ref in refs[:-1]:
        total = total + ref[...].astype(F32)
    out_ref[...] = total * (out_ref.shape[1] ** (-0.5))


def mix_body(bit, yes_ref, no_ref, out_ref):
    picked = (lax.axis_index("kv") & bit) != 0

    @pl.when(picked)
    def _():
        out_ref[...] = yes_ref[...]

    @pl.when(jnp.logical_not(picked))
    def _():
        out_ref[...] = no_ref[...]


def shares_of(tok, m, near, tp):
    share = tok // tp
    if m < 2 or share % 32:
        return [(0, tok)]
    if m < near - 1:
        return [(0, share)]
    return [(0, share // 2), (share // 2, share // 2)]


def cuts(near, far, wanted, x_hbm, out_refs, sem):
    rank = lax.rem(lax.axis_index("kv"), near)
    width = x_hbm.shape[1] // (near * far)
    copies = []
    for index, ((m, first, share), ref) in enumerate(zip(wanted, out_refs)):
        rows = slice(None)
        if share < x_hbm.shape[0]:
            of_plane = x_hbm.shape[0] // lax.axis_size("tp")
            rows = pl.ds(pl.multiple_of(lax.axis_index("tp") * of_plane + first, share), share)
        for z in range(far):
            at = pl.multiple_of((z * near + (rank ^ m)) * width, width)
            copies.append(
                pltpu.make_async_copy(
                    x_hbm.at[rows, pl.ds(at, width)],
                    ref.at[:, z * width : (z + 1) * width],
                    sem.at[index * far + z],
                )
            )
    return copies


def cut_body(near, far, wanted, x_hbm, *refs):
    copies = cuts(near, far, wanted, x_hbm, refs[:-1], refs[-1])
    for copy in copies:
        copy.start()
    for copy in copies:
        copy.wait()


def weight_body(near, far, parity, plan, *refs):
    pieces = refs[: len(plan)]
    rounds_refs, out_ref = refs[len(plan) : -1], refs[-1]
    depth = lax.div(lax.axis_index("kv"), near)
    tok = rounds_refs[0].shape[0]
    width = pieces[0].shape[1] // far
    rights = []
    for m, first, share, turn in plan:
        if share == tok:
            rights.append(rounds_refs[m][...])
            continue
        planes = lax.axis_size("tp")
        at = lax.rem(lax.axis_index("tp") + turn, planes) * (tok // planes) + first
        rights.append(rounds_refs[m][pl.ds(pl.multiple_of(at, share), share), :])
    right = jnp.concatenate(rights, axis=0)
    for index, rel in enumerate(range(parity, far, 2)):
        at = pl.multiple_of((depth ^ rel) * width, width)
        left = jnp.concatenate([piece[:, pl.ds(at, width)] for piece in pieces], axis=0)
        out_ref[index * width : (index + 1) * width, :] = tn(left, right).astype(out_ref.dtype)


def halve_body(blocks, keep_ref, came_ref, rest_ref, send_ref):
    width = keep_ref.shape[0] // blocks
    for block in range(blocks):
        at = slice(block * width, (block + 1) * width)
        to = slice(block // 2 * width, (block // 2 + 1) * width)
        total = keep_ref[at, :] + came_ref[at, :].astype(F32)
        if block % 2:
            send_ref[to, :] = total.astype(BF16)
        else:
            rest_ref[to, :] = total


def add_body(keep_ref, came_ref, out_ref):
    out_ref[...] = keep_ref[...] + came_ref[...].astype(F32)


def per_device(queries, keys, values, attended, out_grad, log_sum, picked, layer_input):
    tok, heads, dim = queries.shape
    sel = picked.shape[1]
    count = lax.axis_size("kv")
    levels = count.bit_length() - 1
    near = 1 << (levels // 2)
    far = count // near
    tp = lax.axis_size("tp")
    rows, _, _, msg_rows = layout(tok, heads, sel)
    flat = lambda x: x.reshape(rows, dim)
    key, value = flat(keys), flat(values)

    def shape(dims, kind):
        return jax.ShapeDtypeStruct(dims, kind)

    pairs = rows * rows * dim * 10
    width = layer_input.shape[1] // count
    blocked = width % 128 == 0 and far > 1
    early = []
    if blocked:
        early = [(m, *part) for m in range(2, near) for part in shares_of(tok, m, near, tp)]
    msg, kv, *first = pl.pallas_call(
        functools.partial(pack_body, levels, heads, near, far, early),
        out_shape=[pltpu.VMEM((msg_rows, dim), BF16), pltpu.VMEM((2 * rows, dim), BF16)]
        + [pltpu.VMEM((part[2], far * width), BF16) for part in early],
        in_specs=[HBM] * 8,
        out_specs=[VMEM] * (2 + len(early)),
        scratch_shapes=[
            pltpu.SMEM(picked.shape, jnp.int32),
            pltpu.VMEM((rows, dim), BF16),
            pltpu.VMEM((heads, tok), F32),
            pltpu.SemaphoreType.DMA((7,)),
            pltpu.SemaphoreType.DMA((max(1, len(early)) * far,)),
        ],
        compiler_params=pltpu.CompilerParams(vmem_limit_bytes=62000000),
    )(picked, flat(queries), flat(out_grad), flat(attended), log_sum.T, layer_input, key, value)
    far_kv = line(kv, 1 << (levels - 1))

    def mix(bit, yes, no):
        return call(
            functools.partial(mix_body, bit), shape(yes.shape, BF16), [VMEM, VMEM], 1 << 18, yes.size * 6
        )(yes, no)

    got = forward(msg, levels, mix)
    if blocked:
        wanted = [(m, 0, tok) for m in (1, 0) if m < near]
        later = pl.pallas_call(
            functools.partial(cut_body, near, far, wanted),
            out_shape=[pltpu.VMEM((tok, far * width), BF16) for _ in wanted],
            in_specs=[HBM],
            out_specs=[VMEM] * len(wanted),
            scratch_shapes=[pltpu.SemaphoreType.DMA((len(wanted) * far,))],
            cost_estimate=pl.CostEstimate(flops=1 << 20, bytes_accessed=layer_input.size, transcendentals=0),
            compiler_params=pltpu.CompilerParams(vmem_limit_bytes=56 << 20),
        )(layer_input)
        cut = dict(zip(early + wanted, first + list(later)))
        pieces, plan = [], []
        for (m, start, share), piece in cut.items():
            if m:
                piece = swap(piece, m)
            pieces.append(piece)
            plan.append((m, start, share, 0))
            if share == tok:
                continue
            for s in range(1, tp):
                pieces.append(lax.ppermute(piece, "tp", [((i + s) % tp, i) for i in range(tp)]))
                plan.append((m, start, share, s))
    dk_own, dv_own, dq_own = call(
        functools.partial(own_body, sel, heads),
        [shape((rows, dim), F32)] * 3,
        [VMEM] * 2,
        pairs, 8 * rows * dim * 4,
    )(msg, kv)

    dq_near = call(
        functools.partial(near_body, sel, heads, levels),
        shape((rows, dim), F32), [VMEM] * 3, pairs * 3 // 5, 8 * rows * dim,
    )(msg, far_kv, dq_own)

    def far_call(groups, dk, dv, last):
        sides = [group for group in groups if group != levels]
        kinds = [shape((rows, dim), BF16)] * len(sides) + [shape((rows, dim), F32)] * 2
        if last:
            kinds.append(shape((tok, heads * dim), BF16))
        return call(
            functools.partial(far_body, sel, heads, groups, last, sides),
            kinds,
            [VMEM] * (len(groups) + 3),
            pairs * len(groups), 8 * rows * dim,
        )(*[got[group - 1] for group in groups], kv, dk, dv)

    back, dk, dv = {}, dk_own, dv_own
    stages = [(3,), (2,), (4,), (1,)] + [(level,) for level in range(5, levels + 1)]
    if levels < 4:
        stages = [tuple(range(1, levels + 1))]
    elif levels > 4:
        stages = [(level,) for level in range(1, levels + 1)]
    for stage in stages:
        outs = far_call(stage, dk, dv, stage == stages[-1])
        sides = [group for group in stage if group != levels]
        for group, side in zip(sides, outs):
            back[group] = ring(side, 1 << (group - 1))
        outs = outs[len(sides) :]
        dk, dv = outs[:2]
    key_grad, value_grad, rounded = outs
    if blocked:
        rounds = {0: rounded}
        bit = near // 2
        while bit:
            for m in list(rounds):
                rounds[m ^ bit] = swap(rounds[m], bit)
            bit //= 2
        columns = heads * dim

        def weight(parity, kind):
            blocks = far // 2
            return call(
                functools.partial(weight_body, near, far, parity, plan),
                shape((blocks * width, columns), kind),
                [VMEM] * (len(pieces) + near),
                2 * near * tok * blocks * width * columns, near * tok * far * width * 2,
            )(*pieces, *[rounds[m] for m in range(near)])

        send = weight(1, BF16)
        total = weight(0, F32)
        bit, left = near, far // 2
        came = swap(send, bit)
        while left > 1:
            bit *= 2
            total, send = call(
                functools.partial(halve_body, left),
                [shape((left // 2 * width, columns), F32), shape((left // 2 * width, columns), BF16)],
                [VMEM] * 2, 1 << 18, left * width * columns * 8,
            )(total, came)
            left //= 2
            came = swap(send, bit)
        total = call(add_body, shape(total.shape, F32), [VMEM] * 2, 1 << 18, total.size * 10, False)(total, came)
    else:
        terms = lax.dot_general(
            layer_input, rounded, (((0,), (0,)), ((), ())), preferred_element_type=F32
        )
        total = lax.psum_scatter(terms, "kv", scatter_dimension=0, tiled=True)
    query_grad = call(
        query_body, shape((rows, dim), F32), [VMEM] * levels, 1 << 20, rows * dim * 16, False
    )(dq_near, *[back[group] for group in range(1, levels)])
    grads = [x.reshape(tok, heads, dim) for x in (query_grad, key_grad, value_grad)]
    return (*grads, total)


def solution(mesh):
    placed = (
        P("kv", "tp", None),
        P("kv", "tp", None),
        P("kv", "tp", None),
        P("kv", "tp", None),
        P("kv", "tp", None),
        P("kv", "tp"),
        P("kv", None),
        P("kv", None),
    )
    return jax.shard_map(
        per_device,
        mesh=mesh,
        in_specs=placed,
        out_specs=(P("kv", "tp", None), P("kv", "tp", None), P("kv", "tp", None), P("kv", "tp")),
        check_vma=False,
    )
```
